32 devices in a mesh: rep: 2 (over x), fs: 8 (over z, y), tp: 2 (over core).
Axes of the slice: x: 2, y: 2, z: 4, core: 2. Of those that a mesh axis runs over, the one named last changes fastest.
Arguments:
- residual: bfloat16 [8192, 2048], P(('rep', 'fs', 'tp')), may hold values from -6 to 6
- mixer_gain: float32 [2048], replicated, may hold values from 0.1 to 1.9
- gating_proj: bfloat16 [2048, 2048], P('fs', 'tp'), may hold values from -0.125 to 0.125
- spatial_proj: bfloat16 [2048, 2048], P('fs', 'tp'), as said below
- spatial_gain: float32 [2048], replicated, may hold values from 0.1 to 1.9
- spatial_bias: float32 [2048], replicated, may hold values from -3 to 3
- spatial_mix: bfloat16 [32, 128, 128], replicated, may hold values from -0.5 to 0.5
- spatial_offset: float32 [32, 128], replicated, may hold values from 0.5 to 1.5
- mixer_out: bfloat16 [2048, 2048], P('tp', 'fs'), may hold values from -0.125 to 0.125
- channel_gain: float32 [2048], replicated, may hold values from 0.1 to 1.9
- gate_proj: bfloat16 [2048, 2816], P('fs', 'tp'), may hold values from -0.125 to 0.125
- up_proj: bfloat16 [2048, 2816], P('fs', 'tp'), may hold values from -0.125 to 0.125
- conv_taps: float32 [3, 2816], replicated, may hold values from -3.5 to 3.5
- down_proj: bfloat16 [2816, 2048], P('tp', 'fs'), may hold values from -0.109375 to 0.109375
Outputs:
- layer_out: bfloat16 [8192, 2048], P(('rep', 'fs', 'tp'))
The draws below stay inside these ranges and needn't reach their ends.
Inputs may be any that keep to these rules, and one draw needn't show every extreme that they name: `spatial_proj`: entries are bounded in magnitude by 56 / sqrt(2048).
All inputs are finite; a program needn't handle non-finite values.
Results may differ from the reference program's by a relative error of at most 0.015.
Values may be sent and summed in bfloat16 or wider, within the bound.
A program may use at most 128 MiB of HBM per device.

```python
import jax
import jax.numpy as jnp
from jax import lax

D = 2048
HEADS = 32
HEAD = 64
GROUP = 2048
BLOCK = 128
SEGMENT = 64
FF = 2816
KCONV = 3
SEQ_LEN = 256
TOKENS = 8192
N_TP = 2


def draw_spatial_proj(key, part):
    key_vals = jax.random.fold_in(key, 11)
    key_cols = jax.random.fold_in(key, 12)
    column = jnp.arange(GROUP).astype(jnp.float32)
    rising = jnp.power(10.0, column / (GROUP - 1))
    jitter = jax.random.uniform(key_cols, (GROUP,), jnp.float32, 0.7, 1.4)
    values = jnp.clip(jax.random.normal(key_vals, (D, GROUP), jnp.float32), -4.0, 4.0)
    return (values * rising * jitter * D ** (-0.5)).astype(jnp.bfloat16)


def level_of(own_key, dims, cuts, smallest, top_value):
    def one(dim, blocks):
        heights = jax.random.uniform(jax.random.fold_in(jax.random.fold_in(own_key, 6), dim), (blocks,), jnp.float32, smallest / len(cuts), top_value / len(cuts))
        return jnp.repeat(jnp.exp(heights), dims[dim] // blocks).reshape((-1,) + (1,) * (len(dims) - dim - 1))

    level = one(*cuts[0])
    for cut in cuts[1:]:
        level = level * one(*cut)
    return level


def bell_draw(own_key, dims, scale, reach, pieces=(), held_as=jnp.bfloat16):
    loudness = level_of(own_key, dims, pieces, -0.22, 0.18) if pieces else 1.0
    drawn = jax.random.normal(own_key, dims, jnp.float32) * scale * loudness
    return jnp.minimum(jnp.maximum(drawn, -reach), reach).astype(held_as)


def setup_inputs(seed: int = 0) -> dict:
    seeds = jax.random.split(jax.random.key(seed), 15)
    residual = bell_draw(seeds[0], (TOKENS, D), 1.0, 6.0, ((0, 32),))
    mixer_gain = jnp.clip(1.0 + 0.18 * jax.random.normal(seeds[1], (D,), jnp.float32), 0.1, 1.9)
    gating_proj = bell_draw(seeds[2], (D, GROUP), D ** -0.5, 0.125, ((0, 8), (1, 2)))
    spatial_proj = draw_spatial_proj(jax.random.fold_in(seeds[14], 71), 0)
    spatial_gain = jnp.clip(1.0 + 0.18 * jax.random.normal(seeds[4], (GROUP,), jnp.float32), 0.1, 1.9)
    spatial_bias = bell_draw(seeds[5], (GROUP,), 0.5, 3.0, (), jnp.float32)
    spatial_mix = bell_draw(seeds[6], (HEADS, BLOCK, BLOCK), BLOCK ** -0.5, 0.5)
    spatial_offset = jnp.clip(jax.random.uniform(seeds[7], (HEADS, BLOCK), jnp.float32, 0.5, 1.5), 0.5, 1.5)
    mixer_out = bell_draw(seeds[8], (GROUP, D), GROUP ** -0.5, 0.125, ((0, 2), (1, 8)))
    channel_gain = jnp.clip(1.0 + 0.18 * jax.random.normal(seeds[9], (D,), jnp.float32), 0.1, 1.9)
    gate_proj = bell_draw(seeds[10], (D, FF), D ** -0.5, 0.125, ((0, 8), (1, 2)))
    up_proj = bell_draw(seeds[11], (D, FF), D ** -0.5, 0.125, ((0, 8), (1, 2)))
    conv_taps = bell_draw(seeds[12], (KCONV, FF), KCONV ** -0.5, 3.5, (), jnp.float32)
    down_proj = bell_draw(seeds[13], (FF, D), FF ** -0.5, 0.109375, ((0, 2), (1, 8)))
    return dict(residual=residual, mixer_gain=mixer_gain, gating_proj=gating_proj, spatial_proj=spatial_proj, spatial_gain=spatial_gain, spatial_bias=spatial_bias, spatial_mix=spatial_mix, spatial_offset=spatial_offset, mixer_out=mixer_out, channel_gain=channel_gain, gate_proj=gate_proj, up_proj=up_proj, conv_taps=conv_taps, down_proj=down_proj)


def round_trip(value):
    return lax.optimization_barrier(value.astype(jnp.bfloat16)).astype(jnp.float32)

def rms_normed(value, gain):
    wide = value.astype(jnp.float32)
    scale = lax.rsqrt(lax.optimization_barrier(jnp.mean(wide * wide, axis=-1, keepdims=True)) + 1e-06)
    return (wide * scale * gain).astype(jnp.bfloat16)

def split_sum(left, right, parts):
    rows, inner = left.shape
    left_parts = left.reshape(rows, parts, inner // parts).astype(jnp.float32)
    right_parts = right.reshape(parts, inner // parts, right.shape[1]).astype(jnp.float32)
    terms = jnp.einsum('snc,ncd->nsd', left_parts, right_parts)
    return lax.optimization_barrier(jnp.sum(terms.astype(jnp.bfloat16).astype(jnp.float32), axis=0))

def one_sequence(args):
    rows, mixer_gain, gating_proj, spatial_proj, spatial_gain, spatial_bias, spatial_mix, spatial_offset, mixer_out, channel_gain, gate_proj, up_proj, conv_taps, down_proj = args
    normed = rms_normed(rows, mixer_gain)
    gating = round_trip(jnp.dot(normed, gating_proj, preferred_element_type=jnp.float32))
    spatial = round_trip(jnp.dot(normed, spatial_proj, preferred_element_type=jnp.float32))
    act_u = jax.nn.gelu(gating)
    act_v = jax.nn.gelu(spatial)
    mean = lax.optimization_barrier(jnp.sum(act_v, axis=-1, keepdims=True)) / GROUP
    var = lax.optimization_barrier(jnp.sum(act_v * act_v, axis=-1, keepdims=True)) / GROUP - mean * mean
    vnorm = ((act_v - mean) * lax.rsqrt(var + 1e-05) * spatial_gain + spatial_bias).astype(jnp.bfloat16)
    place = jnp.arange(BLOCK) // SEGMENT
    allowed = place[None, :] <= place[:, None]
    weights = jnp.where(allowed[None], spatial_mix, jnp.zeros_like(spatial_mix)).astype(jnp.float32)
    blocks = vnorm.reshape(SEQ_LEN // BLOCK, BLOCK, HEADS, HEAD).astype(jnp.float32)
    mixed = jnp.einsum('hij,njhd->nihd', weights, blocks) + spatial_offset.T[None, :, :, None]
    gated = (act_u * mixed.reshape(SEQ_LEN, GROUP)).astype(jnp.bfloat16)
    middle = (rows.astype(jnp.float32) + split_sum(gated, mixer_out, N_TP)).astype(jnp.bfloat16)
    normed2 = rms_normed(middle, channel_gain)
    gate = round_trip(jnp.dot(normed2, gate_proj, preferred_element_type=jnp.float32))
    up = round_trip(jnp.dot(normed2, up_proj, preferred_element_type=jnp.float32))
    padded = jnp.concatenate([jnp.zeros((KCONV - 1, FF), jnp.float32), gate], axis=0)
    conv = jnp.zeros((SEQ_LEN, FF), jnp.float32)
    for tap in range(KCONV):
        conv = conv + conv_taps[tap] * padded[tap:tap + SEQ_LEN]
    hidden = (jax.nn.silu(conv) * up).astype(jnp.bfloat16)
    return (middle.astype(jnp.float32) + split_sum(hidden, down_proj, N_TP)).astype(jnp.bfloat16)

def reference(residual, mixer_gain, gating_proj, spatial_proj, spatial_gain, spatial_bias, spatial_mix, spatial_offset, mixer_out, channel_gain, gate_proj, up_proj, conv_taps, down_proj):
    shaped = residual.reshape(residual.shape[0] // SEQ_LEN, SEQ_LEN, D)

    def apply(rows):
        return one_sequence((rows, mixer_gain, gating_proj, spatial_proj, spatial_gain, spatial_bias, spatial_mix, spatial_offset, mixer_out, channel_gain, gate_proj, up_proj, conv_taps, down_proj))
    result = lax.map(apply, shaped)
    return result.reshape(residual.shape[0], D)
```

```python
import functools

import jax
import jax.numpy as jnp
from jax import lax
from jax.experimental import pallas as pl
from jax.experimental.pallas import tpu as pltpu
from jax.sharding import PartitionSpec as P

HEAD = 64
SEGMENT = 64
KCONV = 3
SEQ_LEN = 256
LANES = 128

MESH = pl.DeviceIdType.MESH
BF16, F32 = jnp.bfloat16, jnp.float32

PHASES = ((0, 1), (2,), (3, 4), (5,))
STREAMS = 6


def dot(a, b):
    return jnp.dot(a, b, preferred_element_type=F32)


def kernel(
    dims,
    residual,
    gating,
    spatial,
    mixer_out,
    gate,
    up,
    down,
    mix,
    mixer_gain,
    channel_gain,
    spatial_gain,
    spatial_bias,
    offset,
    taps,
    out,
    g0,
    g1,
    g2,
    g3,
    g4,
    g5,
    rows_in,
    normed,
    middle,
    act_u,
    act_v,
    gated,
    hidden,
    mixw,
    wcat,
    offs,
    stat,
    part_out,
    part_in,
    sum_out,
    sum_in,
    part_out2,
    part_in2,
    sum_out2,
    sum_in2,
    local_sem,
    recv_sem,
    own_sem,
    z_sem,
    y_sem,
    row_send,
    row_recv,
    stat_send,
    stat_recv,
    part_send,
    part_recv,
    sum_send,
    sum_recv,
    mid_send,
    mid_recv,
    part_send2,
    part_recv2,
    sum_send2,
    sum_recv2,
):
    fs, rows, depth, group, width, units = dims
    lines = fs // 2
    blocks = (g0, g1, g2, g3, g4, g5)
    r, f, c = lax.axis_index("rep"), lax.axis_index("fs"), lax.axis_index("tp")
    q, y = f // 2, f % 2
    mine = c * 2 + r
    beside = c * 2 + 1 - r
    peers = (1 - c) * 2
    left, right = (r, f - 2, c), (r, f + 2, c)
    across, pair = (r, f + 1 - 2 * y, c), (1 - r, f, c)
    twin, diag = (r, f, 1 - c), (1 - r, f, 1 - c)
    has_left, has_right = q > 0, q < lines - 1

    def remote(src, dst, send, recv, device):
        return pltpu.make_async_remote_copy(
            src_ref=src,
            dst_ref=dst,
            send_sem=send,
            recv_sem=recv,
            device_id=device,
            device_id_type=MESH,
        )

    own = (
        gating.at[:, pl.ds(pl.multiple_of(r * width, LANES), width)],
        spatial.at[:, pl.ds(pl.multiple_of(r * width, LANES), width)],
        mixer_out.at[pl.ds(pl.multiple_of(r * width, 16), width)],
        gate,
        up,
        down.at[pl.ds(pl.multiple_of(r * units, 16), units)],
    )
    heads = mixw.shape[0]
    head = mine * heads
    own_copies = [
        pltpu.make_async_copy(own[s], blocks[s].at[f], local_sem.at[s]) for s in range(STREAMS)
    ]
    row_copy = pltpu.make_async_copy(residual, rows_in.at[mine], local_sem.at[STREAMS])
    mix_copy = pltpu.make_async_copy(mix.at[pl.ds(head, heads)], mixw, local_sem.at[STREAMS + 1])
    for copy in own_copies[:2] + [row_copy] + own_copies[2:] + [mix_copy]:
        copy.start()

    barrier = pltpu.get_barrier_semaphore()
    for device in (across, pair, twin, diag):
        pl.semaphore_signal(barrier, inc=1, device_id=device, device_id_type=MESH)

    @pl.when(has_left)
    def _():
        pl.semaphore_signal(barrier, inc=1, device_id=left, device_id_type=MESH)

    @pl.when(has_right)
    def _():
        pl.semaphore_signal(barrier, inc=1, device_id=right, device_id_type=MESH)

    pl.semaphore_wait(barrier, 4 + jnp.minimum(q, 1) + jnp.minimum(lines - 1 - q, 1))

    def block(s, source, send, device):
        ref = blocks[s].at[source]
        return remote(ref, ref, send, recv_sem.at[s, source], device)

    def arrived(s, source):
        block(s, source, y_sem.at[s, source], across).wait_recv()

    def send_own(s):
        own_copies[s].wait()

        @pl.when(has_left)
        def _():
            block(s, f, own_sem.at[s], left).start()

        @pl.when(has_right)
        def _():
            block(s, f, z_sem.at[s, f], right).start()

        block(s, f, y_sem.at[s, f], across).start()

    def step(s, d):
        @pl.when(q - d >= 0)
        def _():
            source = f - 2 * d
            arrived(s, source)

            @pl.when(has_right)
            def _():
                block(s, source, z_sem.at[s, source], right).start()

            block(s, source, y_sem.at[s, source], across).start()

        @pl.when(q + d < lines)
        def _():
            source = f + 2 * d
            arrived(s, source)

            @pl.when(has_left)
            def _():
                block(s, source, z_sem.at[s, source], left).start()

            block(s, source, y_sem.at[s, source], across).start()

    def steps(p, d):
        for s in PHASES[p]:
            step(s, d)

    def crossed(p):
        for s in PHASES[p]:

            @pl.loop(0, lines)
            def _(k):
                arrived(s, 2 * k + 1 - y)

    for s in PHASES[0]:
        send_own(s)
    row_to_pair = remote(
        residual, rows_in.at[mine], row_send.at[0], row_recv.at[mine], pair
    )
    row_to_twin = remote(
        residual, rows_in.at[mine], row_send.at[1], row_recv.at[mine], twin
    )
    row_to_pair.start()
    row_to_twin.start()
    for s in PHASES[1]:
        send_own(s)

    def row_wait(slot):
        remote(
            rows_in.at[slot], rows_in.at[slot], row_send.at[0], row_recv.at[slot], pair
        ).wait_recv()

    tile = 64

    def norm_in(slot):
        @pl.loop(0, rows // tile)
        def _(i):
            here = pl.ds(pl.multiple_of(i * tile, tile), tile)
            wide = rows_in[slot, here, :].astype(F32)
            scale = lax.rsqrt(jnp.mean(wide * wide, axis=-1, keepdims=True) + 1e-06)
            normed[slot, here, :] = (wide * scale * mixer_gain[...]).astype(BF16)

    row_copy.wait()
    norm_in(mine)
    steps(0, 1)
    for s in PHASES[2]:
        send_own(s)
    row_wait(beside)
    row_forward = remote(
        rows_in.at[beside], rows_in.at[beside], row_send.at[2], row_recv.at[beside], twin
    )
    row_forward.start()
    norm_in(beside)
    for j in range(2):
        row_wait(peers + j)
        norm_in(peers + j)

    mix_copy.wait()
    span = mixw.shape[1]
    per = LANES // HEAD
    at_row = lax.broadcasted_iota(jnp.int32, (span, span), 0)
    at_col = lax.broadcasted_iota(jnp.int32, (span, span), 1)
    allowed = at_col // SEGMENT <= at_row // SEGMENT
    eye = at_col == at_row
    lane = lax.broadcasted_iota(jnp.int32, (span, LANES), 1)

    def column_of(row):
        return jnp.sum(
            jnp.where(eye, jnp.broadcast_to(row, (span, span)), 0.0), axis=1, keepdims=True
        )

    def row_of(column):
        return jnp.sum(
            jnp.where(eye, jnp.broadcast_to(column, (span, span)), 0.0), axis=0, keepdims=True
        )

    for p in range(heads // per):
        off = jnp.zeros((span, LANES), F32)
        for k in range(per):
            h = p * per + k
            wcat[p, :, k * span : (k + 1) * span] = jnp.where(
                allowed, mixw[h].astype(F32), 0.0
            ).astype(BF16)
            here = column_of(offset[pl.ds(head + h, 1), :])
            off = jnp.where(lane // HEAD == k, here, off)
        offs[:, p * LANES : (p + 1) * LANES] = off

    for d in range(2, lines):
        steps(0, d)
    crossed(0)

    def project(slot):
        n = normed[slot]
        u = dot(n, g0[...].reshape(depth, width)).astype(BF16).astype(F32)
        act_u[slot] = jax.nn.gelu(u)
        v = jax.nn.gelu(dot(n, g1[...].reshape(depth, width)).astype(BF16).astype(F32))
        act_v[slot] = v
        total = jnp.sum(v, axis=-1, keepdims=True)
        squares = jnp.sum(v * v, axis=-1, keepdims=True)
        for b in range(rows // span):
            here = pl.ds(pl.multiple_of(slot * rows + b * span, LANES), span)
            stat[mine, 0:1, here] = row_of(total[b * span : (b + 1) * span])
            stat[mine, 1:2, here] = row_of(squares[b * span : (b + 1) * span])

    @pl.loop(0, 4)
    def _(slot):
        project(slot)
        for s in PHASES[1]:

            @pl.when(slot + 1 < lines)
            def _():
                step(s, slot + 1)

    for s in PHASES[1]:
        for d in range(5, lines):
            step(s, d)

    stat_copies = [
        remote(stat.at[mine], stat.at[mine], stat_send.at[i], stat_recv.at[mine], device)
        for i, device in enumerate((pair, twin, diag))
    ]
    for copy in stat_copies:
        copy.start()
    for s in PHASES[3]:
        send_own(s)
    for other in (beside, peers, peers + 1):
        remote(
            stat.at[other], stat.at[other], stat_send.at[0], stat_recv.at[other], pair
        ).wait_recv()

    gain_here = spatial_gain[:, pl.ds(pl.multiple_of(mine * width, LANES), width)]
    bias_here = spatial_bias[:, pl.ds(pl.multiple_of(mine * width, LANES), width)]
    pairs = heads // per

    def gate_slot(slot):
        low, high = [], []
        for b in range(rows // span):
            here = pl.ds(pl.multiple_of(slot * rows + b * span, LANES), span)
            sums = stat[0, :, here] + stat[1, :, here] + stat[2, :, here] + stat[3, :, here]
            mean_row = sums[0:1] / group
            var_row = sums[1:2] / group - mean_row * mean_row
            mean = column_of(mean_row)
            scale = lax.rsqrt(column_of(var_row) + 1e-05)
            v = act_v[slot, b * span : (b + 1) * span, :]
            vnorm = (v - mean) * scale * gain_here + bias_here
            parts = []
            for p in range(pairs):
                tile_v = vnorm[:, p * LANES : (p + 1) * LANES]
                parts.append(
                    jnp.concatenate(
                        [
                            jnp.where(lane // HEAD == k, tile_v, 0.0).astype(BF16)
                            for k in range(per)
                        ],
                        axis=0,
                    )
                )
            low.append(parts)
        for p in range(pairs):
            rhs = jnp.concatenate([parts[p] for parts in low], axis=1)
            mixed = dot(wcat[p], rhs)
            here = slice(p * LANES, (p + 1) * LANES)
            for b in range(rows // span):
                there = slice(b * span, (b + 1) * span)
                m = mixed[:, b * LANES : (b + 1) * LANES] + offs[:, here]
                gated[slot, there, here] = (act_u[slot, there, here] * m).astype(BF16)

    @pl.loop(0, 4)
    def _(slot):
        gate_slot(slot)

    crossed(1)

    model = g2.shape[2]

    def product(lhs, weights, k):
        return [dot(lhs, weights[2 * k + j]) for j in range(2)]

    def copy_of(src, dst, send, recv, k, j, device):
        return remote(src.at[k, j], dst.at[k, j], send.at[k, j], recv.at[k, j], device)

    @pl.loop(0, lines)
    def _(k):
        for j in range(2):
            for i, value in enumerate(product(gated[peers + j], g2, k)):
                part_out[k, j, :, i * model : (i + 1) * model] = value.astype(BF16)
            copy_of(part_out, part_in, part_send, part_recv, k, j, twin).start()

    @pl.loop(0, lines)
    def _(k):
        for j in range(2):
            values = product(gated[c * 2 + j], g2, k)
            copy_of(part_out, part_in, part_send, part_recv, k, j, twin).wait_recv()
            for i, value in enumerate(values):
                here = slice(i * model, (i + 1) * model)
                sum_out[k, j, :, here] = (value + part_in[k, j, :, here].astype(F32)).astype(BF16)
            copy_of(sum_out, sum_in, sum_send, sum_recv, k, j, pair).start()

    def mid_copy(k, slot):
        return remote(
            middle.at[k, slot], middle.at[k, slot], mid_send.at[k, slot], mid_recv.at[k, slot], twin
        )

    @pl.loop(0, lines)
    def _(k):
        for j in range(2):
            copy_of(sum_out, sum_in, sum_send, sum_recv, k, j, pair).wait_recv()
            here = pl.ds(pl.multiple_of(k * 2 * model, LANES), 2 * model)
            slot = c * 2 + j
            total = sum_out[k, j].astype(F32) + sum_in[k, j].astype(F32)
            middle[k, slot] = (rows_in[slot, :, here].astype(F32) + total).astype(BF16)
            mid_copy(k, slot).start()

        for s in PHASES[2]:

            @pl.when(k + 1 < lines)
            def _():
                step(s, k + 1)

    def norm_middle(slot):
        @pl.loop(0, rows // tile)
        def _(i):
            here = pl.ds(pl.multiple_of(i * tile, tile), tile)
            wide = [middle[k, slot, here, :].astype(F32) for k in range(lines)]
            total = sum(jnp.sum(w * w, axis=-1, keepdims=True) for w in wide)
            scale = lax.rsqrt(total / depth + 1e-06)
            for k in range(lines):
                there = slice(k * 2 * model, (k + 1) * 2 * model)
                normed[slot, here, there] = (wide[k] * scale * channel_gain[:, there]).astype(BF16)

    for j in range(2):
        norm_middle(c * 2 + j)
    for j in range(2):

        @pl.loop(0, lines)
        def _(k):
            mid_copy(k, peers + j).wait_recv()

        norm_middle(peers + j)

    steps(3, 1)
    crossed(2)

    place = lax.broadcasted_iota(jnp.int32, (rows, units), 0) % SEQ_LEN

    def channel(slot):
        n = normed[slot]
        gates = dot(n, g3[...].reshape(depth, units)).astype(BF16).astype(F32)
        conv = taps[KCONV - 1 : KCONV, :] * gates
        for lag in range(1, KCONV):
            shifted = jnp.where(place >= lag, pltpu.roll(gates, lag, 0), 0.0)
            conv = conv + taps[KCONV - 1 - lag : KCONV - lag, :] * shifted
        ups = dot(n, g4[...].reshape(depth, units)).astype(BF16).astype(F32)
        hidden[slot] = (jax.nn.silu(conv) * ups).astype(BF16)

    @pl.loop(0, 4)
    def _(slot):
        channel(slot)

        @pl.when(slot + 2 < lines)
        def _():
            for s in PHASES[3]:
                step(s, slot + 2)

    for s in PHASES[3]:
        for d in range(6, lines):
            step(s, d)
    crossed(3)

    @pl.loop(0, lines)
    def _(k):
        for j in range(2):
            for i, value in enumerate(product(hidden[peers + j], g5, k)):
                part_out2[k, j, :, i * model : (i + 1) * model] = value.astype(BF16)
            copy_of(part_out2, part_in2, part_send2, part_recv2, k, j, twin).start()

    def sum_copy(k):
        return remote(
            sum_out2.at[k], sum_in2.at[k], sum_send2.at[k], sum_recv2.at[k], pair
        )

    @pl.loop(0, lines)
    def _(k):
        values = product(hidden[beside], g5, k)
        copy_of(part_out2, part_in2, part_send2, part_recv2, k, 1 - r, twin).wait_recv()
        for i, value in enumerate(values):
            here = slice(i * model, (i + 1) * model)
            sum_out2[k, :, here] = (value + part_in2[k, 1 - r, :, here].astype(F32)).astype(BF16)
        sum_copy(k).start()

    @pl.loop(0, lines)
    def _(k):
        values = product(hidden[mine], g5, k)
        copy_of(part_out2, part_in2, part_send2, part_recv2, k, r, twin).wait_recv()
        sum_copy(k).wait_recv()
        for i, value in enumerate(values):
            here = slice(i * model, (i + 1) * model)
            total = value + part_in2[k, r, :, here].astype(F32)
            total = total + sum_in2[k, :, here].astype(F32)
            total = total + middle[k, mine, :, here].astype(F32)
            act = total.astype(BF16)
            for kk in range(lines):

                @pl.when(k == kk)
                def _():
                    at = (2 * kk + i) * model
                    out[:, at : at + model] = act

    for s in range(STREAMS):

        @pl.when(has_left)
        def _():
            block(s, f, own_sem.at[s], left).wait_send()

        @pl.loop(0, lines)
        def _(k):
            source = 2 * k + y
            block(s, source, y_sem.at[s, source], across).wait_send()

            @pl.when(((k <= q) & has_right) | ((k > q) & has_left))
            def _():
                block(s, source, z_sem.at[s, source], across).wait_send()

    for copy in (row_to_pair, row_to_twin, row_forward, *stat_copies):
        copy.wait_send()

    @pl.loop(0, lines)
    def _(k):
        for j in range(2):
            copy_of(part_out, part_in, part_send, part_recv, k, j, twin).wait_send()
            copy_of(sum_out, sum_in, sum_send, sum_recv, k, j, pair).wait_send()
            copy_of(part_out2, part_in2, part_send2, part_recv2, k, j, twin).wait_send()
            mid_copy(k, c * 2 + j).wait_send()
        sum_copy(k).wait_send()


def body(reps, fs, tps):
    assert reps == 2 and tps == 2 and fs % 2 == 0

    def on_device(
        residual,
        mixer_gain,
        gating_proj,
        spatial_proj,
        spatial_gain,
        spatial_bias,
        spatial_mix,
        spatial_offset,
        mixer_out,
        channel_gain,
        gate_proj,
        up_proj,
        conv_taps,
        down_proj,
    ):
        r, c = lax.axis_index("rep"), lax.axis_index("tp")
        rows, depth = residual.shape
        assert rows % SEQ_LEN == 0
        own_rows = gating_proj.shape[0]
        width = gating_proj.shape[1] // reps
        units = gate_proj.shape[1] // reps
        group = gating_proj.shape[1] * tps
        columns = mixer_out.shape[1]
        span = spatial_mix.shape[1]
        heads = width // HEAD
        lines = fs // 2
        gate_here = lax.dynamic_slice_in_dim(gate_proj, r * units, units, 1)
        up_here = lax.dynamic_slice_in_dim(up_proj, r * units, units, 1)
        taps_here = lax.dynamic_slice_in_dim(conv_taps, (c * reps + r) * units, units, 1)
        vmem, hbm = pl.BlockSpec(memory_space=pltpu.VMEM), pl.BlockSpec(memory_space=pl.ANY)
        dma = pltpu.SemaphoreType.DMA
        wide = 2 * columns
        return pl.pallas_call(
            functools.partial(kernel, (fs, rows, depth, group, width, units)),
            out_shape=jax.ShapeDtypeStruct((rows, depth), BF16),
            in_specs=[hbm] * 8 + [vmem] * 6,
            out_specs=vmem,
            scratch_shapes=[
                pltpu.VMEM((fs, own_rows, width), BF16),
                pltpu.VMEM((fs, own_rows, width), BF16),
                pltpu.VMEM((fs, width, columns), BF16),
                pltpu.VMEM((fs, own_rows, units), BF16),
                pltpu.VMEM((fs, own_rows, units), BF16),
                pltpu.VMEM((fs, units, columns), BF16),
                pltpu.VMEM((4, rows, depth), BF16),
                pltpu.VMEM((4, rows, depth), BF16),
                pltpu.VMEM((lines, 4, rows, wide), BF16),
                pltpu.VMEM((4, rows, width), F32),
                pltpu.VMEM((4, rows, width), F32),
                pltpu.VMEM((4, rows, width), BF16),
                pltpu.VMEM((4, rows, units), BF16),
                pltpu.VMEM((heads, span, span), BF16),
                pltpu.VMEM((heads * HEAD // LANES, span, span * LANES // HEAD), BF16),
                pltpu.VMEM((span, width), F32),
                pltpu.VMEM((4, 2, 4 * rows), F32),
                pltpu.VMEM((lines, 2, rows, wide), BF16),
                pltpu.VMEM((lines, 2, rows, wide), BF16),
                pltpu.VMEM((lines, 2, rows, wide), BF16),
                pltpu.VMEM((lines, 2, rows, wide), BF16),
                pltpu.VMEM((lines, 2, rows, wide), BF16),
                pltpu.VMEM((lines, 2, rows, wide), BF16),
                pltpu.VMEM((lines, rows, wide), BF16),
                pltpu.VMEM((lines, rows, wide), BF16),
                dma((STREAMS + 2,)),
                dma((STREAMS, fs)),
                dma((STREAMS,)),
                dma((STREAMS, fs)),
                dma((STREAMS, fs)),
                dma((3,)),
                dma((4,)),
                dma((3,)),
                dma((4,)),
                dma((lines, 2)),
                dma((lines, 2)),
                dma((lines, 2)),
                dma((lines, 2)),
                dma((lines, 4)),
                dma((lines, 4)),
                dma((lines, 2)),
                dma((lines, 2)),
                dma((lines,)),
                dma((lines,)),
            ],
            compiler_params=pltpu.CompilerParams(
                collective_id=0, has_side_effects=True, vmem_limit_bytes=67043328
            ),
        )(
            residual,
            gating_proj,
            spatial_proj,
            mixer_out,
            gate_here,
            up_here,
            down_proj,
            spatial_mix,
            mixer_gain.reshape(1, -1),
            channel_gain.reshape(1, -1),
            spatial_gain.reshape(1, -1),
            spatial_bias.reshape(1, -1),
            spatial_offset,
            taps_here,
        )

    return on_device


def solution(mesh):
    in_specs = (
        P(("rep", "fs", "tp"), None),
        P(),
        P("fs", "tp"),
        P("fs", "tp"),
        P(),
        P(),
        P(),
        P(),
        P("tp", "fs"),
        P(),
        P("fs", "tp"),
        P("fs", "tp"),
        P(),
        P("tp", "fs"),
    )
    out_specs = P(("rep", "fs", "tp"), None)
    return jax.shard_map(
        body(mesh.shape["rep"], mesh.shape["fs"], mesh.shape["tp"]),
        mesh=mesh,
        in_specs=in_specs,
        out_specs=out_specs,
        check_vma=False,
    )
```

```python
import functools

import jax
import jax.numpy as jnp
from jax import lax
from jax.experimental import pallas as pl
from jax.experimental.pallas import tpu as pltpu
from jax.sharding import PartitionSpec as P

HEAD = 64
SEGMENT = 64
KCONV = 3
SEQ_LEN = 256
LANES = 128

MESH = pl.DeviceIdType.MESH
BF16, F32 = jnp.bfloat16, jnp.float32

PHASES = ((0, 1), (2,), (3, 4), (5,))
STREAMS = 6
BY_COPY = (3, 4)


def dot(a, b):
    return jnp.dot(a, b, preferred_element_type=F32)


def kernel(
    dims,
    residual,
    gating,
    spatial,
    mixer_out,
    gate,
    up,
    down,
    mix,
    mixer_gain,
    channel_gain,
    spatial_gain,
    spatial_bias,
    offset,
    taps,
    out,
    g0,
    g1,
    g2,
    g3,
    g4,
    g5,
    raw,
    cross,
    taps_here,
    rows_in,
    normed,
    middle,
    act_u,
    act_v,
    gated,
    hidden,
    mixw,
    wcat,
    offs,
    stat,
    part_out,
    part_in,
    sum_out,
    sum_in,
    last_in,
    local_sem,
    line_recv,
    pair_recv,
    left_send,
    line_send,
    pair_send,
    cross_send,
    row_send,
    row_recv,
    stat_send,
    stat_recv,
    part_send,
    part_recv,
    sum_send,
    sum_recv,
    mid_send,
    mid_recv,
    part_send2,
    part_recv2,
    last_send,
    last_recv,
):
    fs, rows, depth, group, width, units = dims
    lines = fs // 2
    blocks = (g0, g1, g2, g3, g4, g5)
    halves = [block.shape[1] // 2 for block in blocks]
    r, f, c = lax.axis_index("rep"), lax.axis_index("fs"), lax.axis_index("tp")
    q, y = f // 2, f % 2
    beyond = f + 1 - 2 * y
    mine = c * 2 + y
    beside = c * 2 + 1 - y
    peers = (1 - c) * 2
    left, right = (r, f - 2, c), (r, f + 2, c)
    across, copy_chip = (r, beyond, c), (1 - r, f, c)
    twin, diag = (r, f, 1 - c), (r, beyond, 1 - c)
    has_left, has_right = q > 0, q < lines - 1

    def remote(src, dst, send, recv, device):
        return pltpu.make_async_remote_copy(
            src_ref=src,
            dst_ref=dst,
            send_sem=send,
            recv_sem=recv,
            device_id=device,
            device_id_type=MESH,
        )

    def at(start, size, step):
        return pl.ds(pl.multiple_of(start, step), size)

    own_copies = {
        0: (gating.at[:, at(y * width, width, LANES)], g0.at[f]),
        1: (spatial.at[:, at(y * width, width, LANES)], g1.at[f]),
        2: (mixer_out.at[at(y * width, width, 16)], g2.at[f]),
        3: (gate, raw.at[0]),
        4: (up, raw.at[1]),
        5: (down.at[at(y * units, units, 16)], g5.at[f]),
    }
    own_copies = [
        pltpu.make_async_copy(*own_copies[s], local_sem.at[s]) for s in range(STREAMS)
    ]
    heads = mixw.shape[0]
    head = mine * heads
    row_copy = pltpu.make_async_copy(residual, rows_in.at[mine], local_sem.at[STREAMS])
    mix_copy = pltpu.make_async_copy(mix.at[pl.ds(head, heads)], mixw, local_sem.at[STREAMS + 1])
    for copy in own_copies[:2] + [row_copy] + own_copies[2:] + [mix_copy]:
        copy.start()

    barrier = pltpu.get_barrier_semaphore()
    for device in (across, copy_chip, twin, diag):
        pl.semaphore_signal(barrier, inc=1, device_id=device, device_id_type=MESH)

    @pl.when(has_left)
    def _():
        pl.semaphore_signal(barrier, inc=1, device_id=left, device_id_type=MESH)

    @pl.when(has_right)
    def _():
        pl.semaphore_signal(barrier, inc=1, device_id=right, device_id_type=MESH)

    pl.semaphore_wait(barrier, 4 + jnp.minimum(q, 1) + jnp.minimum(lines - 1 - q, 1))

    def half(s, source, h):
        return blocks[s].at[source, at(h * halves[s], halves[s], 16)]

    def on_line(s, source, send, device):
        ref = half(s, source, r)
        return remote(ref, ref, send, line_recv.at[s, source], device)

    def to_copy(s, source):
        ref = half(s, source, r)
        return remote(ref, ref, pair_send.at[s, source], pair_recv.at[s, source], copy_chip)

    def line_wait(s, source):
        on_line(s, source, line_send.at[s, source], across).wait_recv()

    def pair_wait(s, source):
        ref = half(s, source, 1 - r)
        remote(
            ref, ref, pair_send.at[s, source], pair_recv.at[s, source], copy_chip
        ).wait_recv()

    def crossing(s, h):
        start = (1 - y) * width
        here = at(h * halves[s], halves[s], 16)
        if s < 2:
            src = (gating, spatial)[s].at[here, at(start, width, LANES)]
        elif s == 2:
            src = mixer_out.at[at(start + h * halves[s], halves[s], 16)]
        elif s < 5:
            src = cross.at[s - 3, here]
        else:
            src = down.at[at((1 - y) * units + h * halves[s], halves[s], 16)]
        return src, half(s, f, h)

    def cross_line(s):
        src, dst = crossing(s, r)
        return remote(src, dst, cross_send.at[s, 0], line_recv.at[s, f], across)

    def cross_pair(s):
        src, dst = crossing(s, 1 - r)
        return remote(src, dst, cross_send.at[s, 1], pair_recv.at[s, f], across)

    def both_ways(s, source):
        @pl.when(has_left)
        def _():
            on_line(s, source, left_send.at[s, source % 2], left).start()

        @pl.when(has_right)
        def _():
            on_line(s, source, line_send.at[s, source], right).start()

    def own(p):
        for s in PHASES[p]:
            both_ways(s, f)

    def crossed(p):
        for s in PHASES[p]:
            line_wait(s, beyond)
            both_ways(s, beyond)
            if s in BY_COPY:
                to_copy(s, beyond).start()

    def step(s, d, other):
        @pl.when(q - d >= 0)
        def _():
            source = (beyond if other else f) - 2 * d
            line_wait(s, source)

            @pl.when(has_right)
            def _():
                on_line(s, source, line_send.at[s, source], right).start()

            to_copy(s, source).start()

        @pl.when(q + d < lines)
        def _():
            source = (beyond if other else f) + 2 * d
            line_wait(s, source)

            @pl.when(has_left)
            def _():
                on_line(s, source, line_send.at[s, source], left).start()

            to_copy(s, source).start()

    def steps(p, d):
        for other in (False, True):
            for s in PHASES[p]:
                step(s, d, other)

    def complete(s):
        @pl.loop(0, fs)
        def _(source):
            @pl.when(source != f)
            def _():
                pair_wait(s, source)

    row_to_across = remote(residual, rows_in.at[mine], row_send.at[0], row_recv.at[mine], across)
    row_to_twin = remote(residual, rows_in.at[mine], row_send.at[1], row_recv.at[mine], twin)
    for s in PHASES[0] + PHASES[1]:
        cross_line(s).start()
    row_to_across.start()
    row_to_twin.start()
    for s in PHASES[0]:
        cross_pair(s).start()
    for p in range(2):
        for s in PHASES[p]:
            own_copies[s].wait()
        own(p)

    def row_wait(slot):
        remote(
            rows_in.at[slot], rows_in.at[slot], row_send.at[0], row_recv.at[slot], across
        ).wait_recv()

    tile = 64

    def norm_in(slot):
        @pl.loop(0, rows // tile)
        def _(i):
            here = pl.ds(pl.multiple_of(i * tile, tile), tile)
            wide = rows_in[slot, here, :].astype(F32)
            scale = lax.rsqrt(jnp.mean(wide * wide, axis=-1, keepdims=True) + 1e-06)
            normed[slot, here, :] = (wide * scale * mixer_gain[...]).astype(BF16)

    for i, s in enumerate(PHASES[2]):
        own_copies[s].wait()
        for way in range(2):

            @pl.when(y == way)
            def _():
                blocks[s][f] = raw[i, :, way * units : (way + 1) * units]
                cross[i] = raw[i, :, (1 - way) * units : (2 - way) * units]

    for k in range(4):

        @pl.when(mine == k)
        def _():
            taps_here[...] = taps[:, k * units : (k + 1) * units]

    for s in PHASES[2] + PHASES[1] + PHASES[3]:
        if s in PHASES[1]:
            cross_pair(s).start()
        else:
            cross_line(s).start()
    row_copy.wait()
    norm_in(mine)
    own_copies[5].wait()
    mix_copy.wait()

    crossed(0)
    for d in range(1, lines - 1):
        steps(0, d)
    row_wait(beside)
    row_forward = remote(
        rows_in.at[beside], rows_in.at[beside], row_send.at[2], row_recv.at[beside], twin
    )
    row_forward.start()
    norm_in(beside)
    steps(0, lines - 1)
    crossed(1)
    own(2)
    for j in range(2):
        row_wait(peers + j)
        norm_in(peers + j)

    span = mixw.shape[1]
    per = LANES // HEAD
    at_row = lax.broadcasted_iota(jnp.int32, (span, span), 0)
    at_col = lax.broadcasted_iota(jnp.int32, (span, span), 1)
    allowed = at_col // SEGMENT <= at_row // SEGMENT
    eye = at_col == at_row
    lane = lax.broadcasted_iota(jnp.int32, (span, LANES), 1)

    def column_of(row):
        return jnp.sum(
            jnp.where(eye, jnp.broadcast_to(row, (span, span)), 0.0), axis=1, keepdims=True
        )

    def row_of(column):
        return jnp.sum(
            jnp.where(eye, jnp.broadcast_to(column, (span, span)), 0.0), axis=0, keepdims=True
        )

    for p in range(heads // per):
        off = jnp.zeros((span, LANES), F32)
        for k in range(per):
            h = p * per + k
            wcat[p, :, k * span : (k + 1) * span] = jnp.where(
                allowed, mixw[h].astype(F32), 0.0
            ).astype(BF16)
            here = column_of(offset[pl.ds(head + h, 1), :])
            off = jnp.where(lane // HEAD == k, here, off)
        offs[:, p * LANES : (p + 1) * LANES] = off

    for s in PHASES[0]:
        complete(s)

    def project(slot):
        n = normed[slot]
        u = dot(n, g0[...].reshape(depth, width)).astype(BF16).astype(F32)
        act_u[slot] = jax.nn.gelu(u)
        v = jax.nn.gelu(dot(n, g1[...].reshape(depth, width)).astype(BF16).astype(F32))
        act_v[slot] = v
        total = jnp.sum(v, axis=-1, keepdims=True)
        squares = jnp.sum(v * v, axis=-1, keepdims=True)
        for b in range(rows // span):
            here = pl.ds(pl.multiple_of(slot * rows + b * span, LANES), span)
            stat[mine, 0:1, here] = row_of(total[b * span : (b + 1) * span])
            stat[mine, 1:2, here] = row_of(squares[b * span : (b + 1) * span])

    @pl.loop(0, 4)
    def _(slot):
        project(slot)

        @pl.when(slot + 1 < lines)
        def _():
            steps(1, slot + 1)

    for d in range(5, lines):
        steps(1, d)

    stat_copies = [
        remote(stat.at[mine], stat.at[mine], stat_send.at[i], stat_recv.at[mine], device)
        for i, device in enumerate((across, twin, diag))
    ]
    for copy in stat_copies:
        copy.start()
    crossed(2)
    own(3)
    for other in (beside, peers, peers + 1):
        remote(
            stat.at[other], stat.at[other], stat_send.at[0], stat_recv.at[other], across
        ).wait_recv()

    gain_here = spatial_gain[:, pl.ds(pl.multiple_of(mine * width, LANES), width)]
    bias_here = spatial_bias[:, pl.ds(pl.multiple_of(mine * width, LANES), width)]
    pairs = heads // per

    def gate_slot(slot):
        low = []
        for b in range(rows // span):
            here = pl.ds(pl.multiple_of(slot * rows + b * span, LANES), span)
            sums = stat[0, :, here] + stat[1, :, here] + stat[2, :, here] + stat[3, :, here]
            mean_row = sums[0:1] / group
            var_row = sums[1:2] / group - mean_row * mean_row
            mean = column_of(mean_row)
            scale = lax.rsqrt(column_of(var_row) + 1e-05)
            v = act_v[slot, b * span : (b + 1) * span, :]
            vnorm = (v - mean) * scale * gain_here + bias_here
            parts = []
            for p in range(pairs):
                tile_v = vnorm[:, p * LANES : (p + 1) * LANES]
                parts.append(
                    jnp.concatenate(
                        [
                            jnp.where(lane // HEAD == k, tile_v, 0.0).astype(BF16)
                            for k in range(per)
                        ],
                        axis=0,
                    )
                )
            low.append(parts)
        for p in range(pairs):
            rhs = jnp.concatenate([parts[p] for parts in low], axis=1)
            mixed = dot(wcat[p], rhs)
            here = slice(p * LANES, (p + 1) * LANES)
            for b in range(rows // span):
                there = slice(b * span, (b + 1) * span)
                m = mixed[:, b * LANES : (b + 1) * LANES] + offs[:, here]
                gated[slot, there, here] = (act_u[slot, there, here] * m).astype(BF16)

    @pl.loop(0, 4)
    def _(slot):
        gate_slot(slot)

    model = g2.shape[2]
    near = jnp.minimum(q, lines - 1 - q)

    def nth(i):
        d = (i + 1) // 2
        close = jnp.where(i % 2 == 1, q + d, q - d)
        far = jnp.where(q < lines - 1 - q, i, lines - 1 - i)
        return jnp.where(i <= 2 * near, close, far)

    def of_unit(i):
        k = nth(i)
        return 2 * k + y, 2 * k + 1 - y

    def part_copy(b):
        return remote(part_out.at[b], part_in.at[b], part_send.at[b], part_recv.at[b], twin)

    def sum_copy(b):
        return remote(sum_out.at[b], sum_in.at[b], sum_send.at[b], sum_recv.at[b], across)

    def mid_copy(k, slot):
        return remote(
            middle.at[k, slot], middle.at[k, slot], mid_send.at[k, slot], mid_recv.at[k, slot], twin
        )

    def mixer_product(first, b):
        lhs = gated[pl.ds(first, 2)].reshape(2 * rows, width)
        return dot(lhs, g2[b]).reshape(2, rows, model)

    @pl.loop(0, lines + 1)
    def _(i):
        @pl.when(i < lines)
        def _():
            for b in of_unit(i):

                @pl.when(b != f)
                def _():
                    pair_wait(2, b)

                part_out[b] = mixer_product(peers, b).astype(BF16)
                part_copy(b).start()

        @pl.when(i > 0)
        def _():
            for b in of_unit(i - 1):
                value = mixer_product(c * 2, b)
                part_copy(b).wait_recv()
                sum_out[b] = (value + part_in[b].astype(F32)).astype(BF16)
                sum_copy(b).start()

    for s in PHASES[3]:
        cross_pair(s).start()

    @pl.loop(0, lines)
    def _(i):
        @pl.when(i + 1 < lines)
        def _():
            steps(2, i + 1)

        @pl.when(i == lines - 2)
        def _():
            crossed(3)

        @pl.when(i == lines - 1)
        def _():
            steps(3, 1)

        k = nth(i)
        here = pl.ds(pl.multiple_of(k * 2 * model, LANES), 2 * model)
        for side in range(2):
            b = 2 * k + side
            sum_copy(b).wait_recv()
            for j in range(2):
                slot = c * 2 + j
                there = slice(side * model, (side + 1) * model)
                base = rows_in[slot, :, here][:, there].astype(F32)
                total = sum_out[b, j].astype(F32) + sum_in[b, j].astype(F32)
                middle[k, slot, :, there] = (base + total).astype(BF16)
        for j in range(2):
            mid_copy(k, c * 2 + j).start()

    def norm_middle(slot):
        @pl.loop(0, rows // tile)
        def _(i):
            here = pl.ds(pl.multiple_of(i * tile, tile), tile)
            wide = [middle[k, slot, here, :].astype(F32) for k in range(lines)]
            total = sum(jnp.sum(w * w, axis=-1, keepdims=True) for w in wide)
            scale = lax.rsqrt(total / depth + 1e-06)
            for k in range(lines):
                there = slice(k * 2 * model, (k + 1) * 2 * model)
                normed[slot, here, there] = (wide[k] * scale * channel_gain[:, there]).astype(BF16)

    for j in range(2):
        norm_middle(c * 2 + j)
    for j in range(2):

        @pl.loop(0, lines)
        def _(k):
            mid_copy(k, peers + j).wait_recv()

        norm_middle(peers + j)

    for s in PHASES[2]:
        complete(s)

    place = lax.broadcasted_iota(jnp.int32, (rows, units), 0) % SEQ_LEN

    def channel(slot):
        n = normed[slot]
        gates = dot(n, g3[...].reshape(depth, units)).astype(BF16).astype(F32)
        conv = taps_here[KCONV - 1 : KCONV, :] * gates
        for lag in range(1, KCONV):
            shifted = jnp.where(place >= lag, pltpu.roll(gates, lag, 0), 0.0)
            conv = conv + taps_here[KCONV - 1 - lag : KCONV - lag, :] * shifted
        ups = dot(n, g4[...].reshape(depth, units)).astype(BF16).astype(F32)
        hidden[slot] = (jax.nn.silu(conv) * ups).astype(BF16)

    def half_channel(side):
        @pl.loop(0, 2)
        def _(core):
            channel(core * 2 + side)

    @pl.loop(0, fs)
    def _(b):
        part_copy(b).wait_send()
        sum_copy(b).wait_send()

    def last_part(b, side):
        return remote(
            part_out.at[b, side],
            part_in.at[b, side],
            part_send2.at[b, side],
            part_recv2.at[b, side],
            twin,
        )

    def last_copy(b):
        return remote(sum_out.at[b, 0], last_in.at[b], last_send.at[b], last_recv.at[b], across)

    def give(b, side):
        part_out[b, side] = dot(hidden[peers + side], g5[b]).astype(BF16)
        last_part(b, side).start()

    def send_units(first, last):
        @pl.loop(first, last + 1)
        def _(i):
            @pl.when(i < last)
            def _():
                for b in of_unit(i):

                    @pl.when(b != f)
                    def _():
                        pair_wait(5, b)

                    give(b, 1 - y)

            @pl.when(i > first)
            def _():
                for b in of_unit(i - 1):
                    value = dot(hidden[beside], g5[b])
                    last_part(b, 1 - y).wait_recv()
                    sum_out[b, 0] = (value + part_in[b, 1 - y].astype(F32)).astype(BF16)
                    last_copy(b).start()

    half_channel(1 - y)
    split = lines // 2
    reach = min(lines, max(split, 3))
    for d in range(2, reach):
        steps(3, d)
    send_units(0, split)
    half_channel(y)
    for d in range(reach, lines):
        steps(3, d)
    send_units(split, lines)

    @pl.loop(0, lines)
    def _(i):
        for b in of_unit(i):
            give(b, y)

    @pl.loop(0, lines)
    def _(i):
        k = nth(i)
        values = [dot(hidden[mine], g5[2 * k + side]) for side in range(2)]
        for side in range(2):
            b = 2 * k + side
            last_part(b, y).wait_recv()
            last_copy(b).wait_recv()
            total = values[side] + part_in[b, y].astype(F32) + last_in[b].astype(F32)
            there = slice(side * model, (side + 1) * model)
            values[side] = (total + middle[k, mine, :, there].astype(F32)).astype(BF16)
        here = pl.ds(pl.multiple_of(k * 2 * model, LANES), 2 * model)
        out[:, here] = jnp.concatenate(values, axis=1)

    for s in range(STREAMS):
        cross_line(s).wait_send()
        if s in BY_COPY:
            to_copy(s, beyond).wait_send()
        else:
            cross_pair(s).wait_send()

        @pl.when(has_left)
        def _():
            for side in range(2):
                on_line(s, 2 * q + side, left_send.at[s, side], left).wait_send()

        @pl.loop(0, fs)
        def _(source):
            k = source // 2

            @pl.when(((k <= q) & has_right) | ((k > q) & has_left))
            def _():
                on_line(s, source, line_send.at[s, source], across).wait_send()

            @pl.when(k != q)
            def _():
                to_copy(s, source).wait_send()

    for copy in (row_to_across, row_to_twin, row_forward, *stat_copies):
        copy.wait_send()

    @pl.loop(0, fs)
    def _(b):
        for side in range(2):
            last_part(b, side).wait_send()
        last_copy(b).wait_send()

    @pl.loop(0, lines)
    def _(k):
        for j in range(2):
            mid_copy(k, c * 2 + j).wait_send()


def body(reps, fs, tps):
    assert reps == 2 and tps == 2 and fs % 2 == 0

    def on_device(
        residual,
        mixer_gain,
        gating_proj,
        spatial_proj,
        spatial_gain,
        spatial_bias,
        spatial_mix,
        spatial_offset,
        mixer_out,
        channel_gain,
        gate_proj,
        up_proj,
        conv_taps,
        down_proj,
    ):
        rows, depth = residual.shape
        assert rows % SEQ_LEN == 0
        own_rows = gating_proj.shape[0]
        width = gating_proj.shape[1] // 2
        units = gate_proj.shape[1] // 2
        group = gating_proj.shape[1] * tps
        columns = mixer_out.shape[1]
        span = spatial_mix.shape[1]
        heads = width // HEAD
        lines = fs // 2
        vmem, hbm = pl.BlockSpec(memory_space=pltpu.VMEM), pl.BlockSpec(memory_space=pl.ANY)
        dma = pltpu.SemaphoreType.DMA
        return pl.pallas_call(
            functools.partial(kernel, (fs, rows, depth, group, width, units)),
            out_shape=jax.ShapeDtypeStruct((rows, depth), BF16),
            in_specs=[hbm] * 8 + [vmem] * 6,
            out_specs=vmem,
            scratch_shapes=[
                pltpu.VMEM((fs, own_rows, width), BF16),
                pltpu.VMEM((fs, own_rows, width), BF16),
                pltpu.VMEM((fs, width, columns), BF16),
                pltpu.VMEM((fs, own_rows, units), BF16),
                pltpu.VMEM((fs, own_rows, units), BF16),
                pltpu.VMEM((fs, units, columns), BF16),
                pltpu.VMEM((2, own_rows, 2 * units), BF16),
                pltpu.VMEM((2, own_rows, units), BF16),
                pltpu.VMEM((KCONV, units), F32),
                pltpu.VMEM((4, rows, depth), BF16),
                pltpu.VMEM((4, rows, depth), BF16),
                pltpu.VMEM((lines, 4, rows, 2 * columns), BF16),
                pltpu.VMEM((4, rows, width), F32),
                pltpu.VMEM((4, rows, width), F32),
                pltpu.VMEM((4, rows, width), BF16),
                pltpu.VMEM((4, rows, units), BF16),
                pltpu.VMEM((heads, span, span), BF16),
                pltpu.VMEM((heads * HEAD // LANES, span, span * LANES // HEAD), BF16),
                pltpu.VMEM((span, width), F32),
                pltpu.VMEM((4, 2, 4 * rows), F32),
                pltpu.VMEM((fs, 2, rows, columns), BF16),
                pltpu.VMEM((fs, 2, rows, columns), BF16),
                pltpu.VMEM((fs, 2, rows, columns), BF16),
                pltpu.VMEM((fs, 2, rows, columns), BF16),
                pltpu.VMEM((fs, rows, columns), BF16),
                dma((STREAMS + 2,)),
                dma((STREAMS, fs)),
                dma((STREAMS, fs)),
                dma((STREAMS, 2)),
                dma((STREAMS, fs)),
                dma((STREAMS, fs)),
                dma((STREAMS, 2)),
                dma((3,)),
                dma((4,)),
                dma((3,)),
                dma((4,)),
                dma((fs,)),
                dma((fs,)),
                dma((fs,)),
                dma((fs,)),
                dma((lines, 4)),
                dma((lines, 4)),
                dma((fs, 2)),
                dma((fs, 2)),
                dma((fs,)),
                dma((fs,)),
            ],
            compiler_params=pltpu.CompilerParams(
                collective_id=0, has_side_effects=True, vmem_limit_bytes=67043328
            ),
        )(
            residual,
            gating_proj,
            spatial_proj,
            mixer_out,
            gate_proj,
            up_proj,
            down_proj,
            spatial_mix,
            mixer_gain.reshape(1, -1),
            channel_gain.reshape(1, -1),
            spatial_gain.reshape(1, -1),
            spatial_bias.reshape(1, -1),
            spatial_offset,
            conv_taps,
        )

    return on_device


def solution(mesh):
    in_specs = (
        P(("rep", "fs", "tp"), None),
        P(),
        P("fs", "tp"),
        P("fs", "tp"),
        P(),
        P(),
        P(),
        P(),
        P("tp", "fs"),
        P(),
        P("fs", "tp"),
        P("fs", "tp"),
        P(),
        P("tp", "fs"),
    )
    out_specs = P(("rep", "fs", "tp"), None)
    return jax.shard_map(
        body(mesh.shape["rep"], mesh.shape["fs"], mesh.shape["tp"]),
        mesh=mesh,
        in_specs=in_specs,
        out_specs=out_specs,
        check_vma=False,
    )
```

```python
import functools

import jax
import jax.numpy as jnp
from jax import lax
from jax.experimental import pallas as pl
from jax.experimental.pallas import tpu as pltpu
from jax.sharding import PartitionSpec as P

HEAD = 64
SEGMENT = 64
KCONV = 3
SEQ_LEN = 256
LANES = 128

MESH = pl.DeviceIdType.MESH
BF16, F32 = jnp.bfloat16, jnp.float32

PHASES = ((0, 1), (2,), (3, 4), (5,))
STREAMS = 6
BY_COPY = (0, 1)


def dot(a, b):
    return jnp.dot(a, b, preferred_element_type=F32)


def kernel(
    dims,
    residual,
    gating,
    spatial,
    mixer_out,
    gate,
    up,
    down,
    mix,
    mixer_gain,
    channel_gain,
    spatial_gain,
    spatial_bias,
    offset,
    taps,
    out,
    g0,
    g1,
    g2,
    g34,
    g5,
    raw,
    cross,
    taps_here,
    rows_in,
    normed,
    middle,
    act_u,
    act_v,
    gated,
    hidden,
    mixw,
    wcat,
    offs,
    stat,
    part_out,
    part_in,
    sum_out,
    sum_in,
    last_in,
    out_here,
    local_sem,
    out_sem,
    line_recv,
    pair_recv,
    left_send,
    line_send,
    pair_send,
    cross_send,
    row_send,
    row_recv,
    stat_send,
    stat_recv,
    part_send,
    part_recv,
    sum_send,
    sum_recv,
    mid_send,
    mid_recv,
    part_send2,
    part_recv2,
    last_send,
    last_recv,
):
    fs, rows, depth, group, width, units = dims
    lines = fs // 2
    blocks = (g0, g1, g2, g34, g34, g5)
    halves = [block.shape[1] // 2 for block in blocks]
    sizes = [size // 2 if s in PHASES[2] else size for s, size in enumerate(halves)]
    starts = [sizes[s] if s == PHASES[2][1] else 0 for s in range(STREAMS)]
    r, f, c = lax.axis_index("rep"), lax.axis_index("fs"), lax.axis_index("tp")
    q, y = f // 2, f % 2
    beyond = f + 1 - 2 * y
    mine = c * 2 + y
    beside = c * 2 + 1 - y
    peers = (1 - c) * 2
    left, right = (r, f - 2, c), (r, f + 2, c)
    across, copy_chip = (r, beyond, c), (1 - r, f, c)
    twin, diag = (r, f, 1 - c), (r, beyond, 1 - c)
    has_left, has_right = q > 0, q < lines - 1

    def remote(src, dst, send, recv, device):
        return pltpu.make_async_remote_copy(
            src_ref=src,
            dst_ref=dst,
            send_sem=send,
            recv_sem=recv,
            device_id=device,
            device_id_type=MESH,
        )

    def at(start, size, step):
        return pl.ds(pl.multiple_of(start, step), size)

    own_copies = {
        0: (gating.at[:, at(y * width, width, LANES)], g0.at[f]),
        1: (spatial.at[:, at(y * width, width, LANES)], g1.at[f]),
        2: (mixer_out.at[at(y * width, width, 16)], g2.at[f]),
        3: (gate, raw.at[0]),
        4: (up, raw.at[1]),
        5: (down.at[at(y * units, units, 16)], g5.at[f]),
    }
    own_copies = [
        pltpu.make_async_copy(*own_copies[s], local_sem.at[s]) for s in range(STREAMS)
    ]
    heads = mixw.shape[0]
    head = mine * heads
    row_copy = pltpu.make_async_copy(residual, rows_in.at[mine], local_sem.at[STREAMS])
    mix_copy = pltpu.make_async_copy(mix.at[pl.ds(head, heads)], mixw, local_sem.at[STREAMS + 1])
    for copy in own_copies[:2] + [row_copy] + own_copies[2:] + [mix_copy]:
        copy.start()

    barrier = pltpu.get_barrier_semaphore()
    for device in (across, copy_chip, twin, diag):
        pl.semaphore_signal(barrier, inc=1, device_id=device, device_id_type=MESH)

    @pl.when(has_left)
    def _():
        pl.semaphore_signal(barrier, inc=1, device_id=left, device_id_type=MESH)

    @pl.when(has_right)
    def _():
        pl.semaphore_signal(barrier, inc=1, device_id=right, device_id_type=MESH)

    pl.semaphore_wait(barrier, 4 + jnp.minimum(q, 1) + jnp.minimum(lines - 1 - q, 1))

    def half(s, source, h):
        return blocks[s].at[source, at(h * halves[s] + starts[s], sizes[s], 16)]

    def on_line(s, source, send, device):
        ref = half(s, source, r)
        return remote(ref, ref, send, line_recv.at[s, source], device)

    def to_copy(s, source):
        ref = half(s, source, r)
        return remote(ref, ref, pair_send.at[s, source], pair_recv.at[s, source], copy_chip)

    def line_wait(s, source):
        on_line(s, source, line_send.at[s, source], across).wait_recv()

    def pair_wait(s, source):
        ref = half(s, source, 1 - r)
        remote(
            ref, ref, pair_send.at[s, source], pair_recv.at[s, source], copy_chip
        ).wait_recv()

    def crossing(s, h):
        start = (1 - y) * width
        here = at(h * halves[s], halves[s], 16)
        if s < 2:
            src = (gating, spatial)[s].at[here, at(start, width, LANES)]
        elif s == 2:
            src = mixer_out.at[at(start + h * halves[s], halves[s], 16)]
        elif s < 5:
            src = cross.at[at(h * halves[s] + starts[s], sizes[s], 16)]
        else:
            src = down.at[at((1 - y) * units + h * halves[s], halves[s], 16)]
        return src, half(s, f, h)

    def cross_line(s):
        src, dst = crossing(s, r)
        return remote(src, dst, cross_send.at[s, 0], line_recv.at[s, f], across)

    def cross_pair(s):
        src, dst = crossing(s, 1 - r)
        return remote(src, dst, cross_send.at[s, 1], pair_recv.at[s, f], across)

    def both_ways(s, source):
        @pl.when(has_left)
        def _():
            on_line(s, source, left_send.at[s, source % 2], left).start()

        @pl.when(has_right)
        def _():
            on_line(s, source, line_send.at[s, source], right).start()

    def own(p):
        for s in PHASES[p]:
            both_ways(s, f)

    def crossed(p):
        for s in PHASES[p]:
            line_wait(s, beyond)
            both_ways(s, beyond)
            if s in BY_COPY:
                to_copy(s, beyond).start()

    near = jnp.minimum(q, lines - 1 - q)
    at_end, inside = near == 0, near > 0

    def step(s, d, other, who):
        @pl.when((q - d >= 0) & who)
        def _():
            source = (beyond if other else f) - 2 * d
            line_wait(s, source)

            @pl.when(has_right)
            def _():
                on_line(s, source, line_send.at[s, source], right).start()

            to_copy(s, source).start()

        @pl.when((q + d < lines) & who)
        def _():
            source = (beyond if other else f) + 2 * d
            line_wait(s, source)

            @pl.when(has_left)
            def _():
                on_line(s, source, line_send.at[s, source], left).start()

            to_copy(s, source).start()

    def steps(p, d, who=True, others=(False, True)):
        for other in others:
            for s in PHASES[p]:
                step(s, d, other, who)

    def steps_from(p, first, who):
        for d in range(first, lines):
            steps(p, d, who)

    def complete(s):
        @pl.loop(0, fs)
        def _(source):
            @pl.when(source != f)
            def _():
                pair_wait(s, source)

    row_to_across = remote(residual, rows_in.at[mine], row_send.at[0], row_recv.at[mine], across)
    row_to_twin = remote(residual, rows_in.at[mine], row_send.at[1], row_recv.at[mine], twin)
    for s in PHASES[0] + PHASES[1]:
        cross_line(s).start()
    row_to_across.start()
    row_to_twin.start()
    for s in PHASES[0]:
        own_copies[s].wait()
    own(0)

    def row_wait(slot):
        remote(
            rows_in.at[slot], rows_in.at[slot], row_send.at[0], row_recv.at[slot], across
        ).wait_recv()

    tile = 64

    def norm_in(slot):
        @pl.loop(0, rows // tile)
        def _(i):
            here = pl.ds(pl.multiple_of(i * tile, tile), tile)
            wide = rows_in[slot, here, :].astype(F32)
            scale = lax.rsqrt(jnp.mean(wide * wide, axis=-1, keepdims=True) + 1e-06)
            normed[slot, here, :] = (wide * scale * mixer_gain[...]).astype(BF16)

    main = units // LANES * LANES
    rest = units - main
    for s in PHASES[2]:
        own_copies[s].wait()
    for way in range(2):

        @pl.when(y == way)
        def _():
            for i in range(2):
                for ref, first in ((g34.at[f], way * units), (cross, (1 - way) * units)):
                    ref[:, i * main : (i + 1) * main] = raw[i, :, first : first + main]
                    if rest:
                        there = slice(2 * main + i * rest, 2 * main + (i + 1) * rest)
                        ref[:, there] = raw[i, :, first + main : first + units]

    for k in range(4):

        @pl.when(mine == k)
        def _():
            taps_here[...] = taps[:, k * units : (k + 1) * units]

    row_copy.wait()
    norm_in(mine)
    own_copies[2].wait()
    own_copies[5].wait()
    mix_copy.wait()

    crossed(0)
    for d in range(1, lines - 1):
        steps(0, d)
    own(1)
    crossed(1)
    for s in PHASES[2]:
        cross_line(s).start()
    steps(0, lines - 1)
    row_wait(beside)
    row_forward = remote(
        rows_in.at[beside], rows_in.at[beside], row_send.at[2], row_recv.at[beside], twin
    )
    row_forward.start()
    norm_in(beside)
    for s in PHASES[1] + PHASES[2]:
        cross_pair(s).start()
    steps(1, 1)
    steps_from(1, 2, inside)
    own(2)
    for j in range(2):
        row_wait(peers + j)
        norm_in(peers + j)

    span = mixw.shape[1]
    per = LANES // HEAD
    at_row = lax.broadcasted_iota(jnp.int32, (span, span), 0)
    at_col = lax.broadcasted_iota(jnp.int32, (span, span), 1)
    allowed = at_col // SEGMENT <= at_row // SEGMENT
    eye = at_col == at_row
    lane = lax.broadcasted_iota(jnp.int32, (span, LANES), 1)

    def column_of(row):
        return jnp.sum(
            jnp.where(eye, jnp.broadcast_to(row, (span, span)), 0.0), axis=1, keepdims=True
        )

    def row_of(column):
        return jnp.sum(
            jnp.where(eye, jnp.broadcast_to(column, (span, span)), 0.0), axis=0, keepdims=True
        )

    for p in range(heads // per):
        off = jnp.zeros((span, LANES), F32)
        for k in range(per):
            h = p * per + k
            wcat[p, :, k * span : (k + 1) * span] = jnp.where(
                allowed, mixw[h].astype(F32), 0.0
            ).astype(BF16)
            here = column_of(offset[pl.ds(head + h, 1), :])
            off = jnp.where(lane // HEAD == k, here, off)
        offs[:, p * LANES : (p + 1) * LANES] = off

    for s in PHASES[0]:
        complete(s)

    def project(slot):
        n = normed[slot]
        u = dot(n, g0[...].reshape(depth, width)).astype(BF16).astype(F32)
        act_u[slot] = jax.nn.gelu(u)
        v = jax.nn.gelu(dot(n, g1[...].reshape(depth, width)).astype(BF16).astype(F32))
        act_v[slot] = v
        total = jnp.sum(v, axis=-1, keepdims=True)
        squares = jnp.sum(v * v, axis=-1, keepdims=True)
        for b in range(rows // span):
            here = pl.ds(pl.multiple_of(slot * rows + b * span, LANES), span)
            stat[mine, 0:1, here] = row_of(total[b * span : (b + 1) * span])
            stat[mine, 1:2, here] = row_of(squares[b * span : (b + 1) * span])

    last = lines - 1

    @pl.loop(0, 4)
    def _(slot):
        project(slot)

        @pl.when(slot == 1)
        def _():
            crossed(2)
            for d in range(2, last):
                steps(1, d, at_end, (False,))

        @pl.when(slot == 2)
        def _():
            for d in range(2, last):
                steps(1, d, at_end, (True,))

    stat_copies = [
        remote(stat.at[mine], stat.at[mine], stat_send.at[i], stat_recv.at[mine], device)
        for i, device in enumerate((across, twin, diag))
    ]
    for copy in stat_copies:
        copy.start()
    for s in PHASES[3]:
        cross_line(s).start()
    steps(1, last, at_end & (last > 1))
    for other in (beside, peers, peers + 1):
        remote(
            stat.at[other], stat.at[other], stat_send.at[0], stat_recv.at[other], across
        ).wait_recv()

    gain_here = spatial_gain[:, pl.ds(pl.multiple_of(mine * width, LANES), width)]
    bias_here = spatial_bias[:, pl.ds(pl.multiple_of(mine * width, LANES), width)]
    pairs = heads // per

    def gate_slot(slot):
        low = []
        for b in range(rows // span):
            here = pl.ds(pl.multiple_of(slot * rows + b * span, LANES), span)
            sums = stat[0, :, here] + stat[1, :, here] + stat[2, :, here] + stat[3, :, here]
            mean_row = sums[0:1] / group
            var_row = sums[1:2] / group - mean_row * mean_row
            mean = column_of(mean_row)
            scale = lax.rsqrt(column_of(var_row) + 1e-05)
            v = act_v[slot, b * span : (b + 1) * span, :]
            vnorm = (v - mean) * scale * gain_here + bias_here
            parts = []
            for p in range(pairs):
                tile_v = vnorm[:, p * LANES : (p + 1) * LANES]
                parts.append(
                    jnp.concatenate(
                        [
                            jnp.where(lane // HEAD == k, tile_v, 0.0).astype(BF16)
                            for k in range(per)
                        ],
                        axis=0,
                    )
                )
            low.append(parts)
        for p in range(pairs):
            rhs = jnp.concatenate([parts[p] for parts in low], axis=1)
            mixed = dot(wcat[p], rhs)
            here = slice(p * LANES, (p + 1) * LANES)
            for b in range(rows // span):
                there = slice(b * span, (b + 1) * span)
                m = mixed[:, b * LANES : (b + 1) * LANES] + offs[:, here]
                gated[slot, there, here] = (act_u[slot, there, here] * m).astype(BF16)

    @pl.loop(0, 4)
    def _(slot):
        gate_slot(slot)

    model = g2.shape[2]
    def nth(i):
        d = (i + 1) // 2
        close = jnp.where(i % 2 == 1, q + d, q - d)
        far = jnp.where(q < lines - 1 - q, i, lines - 1 - i)
        return jnp.where(i <= 2 * near, close, far)

    def of_unit(i):
        k = nth(i)
        return 2 * k + y, 2 * k + 1 - y

    def part_copy(b):
        return remote(part_out.at[b], part_in.at[b], part_send.at[b], part_recv.at[b], twin)

    def sum_copy(b):
        return remote(sum_out.at[b], sum_in.at[b], sum_send.at[b], sum_recv.at[b], across)

    def mid_copy(k, slot):
        return remote(
            middle.at[k, slot], middle.at[k, slot], mid_send.at[k, slot], mid_recv.at[k, slot], twin
        )

    def mixer_product(first, b):
        lhs = gated[pl.ds(first, 2)].reshape(2 * rows, width)
        return dot(lhs, g2[b]).reshape(2, rows, model)

    @pl.loop(0, lines + 1)
    def _(i):
        @pl.when(i < lines)
        def _():
            for b in of_unit(i):

                @pl.when(b != f)
                def _():
                    pair_wait(2, b)

                part_out[b] = mixer_product(peers, b).astype(BF16)
                part_copy(b).start()

        @pl.when(i > 0)
        def _():
            for b in of_unit(i - 1):
                value = mixer_product(c * 2, b)
                part_copy(b).wait_recv()
                sum_out[b] = (value + part_in[b].astype(F32)).astype(BF16)
                sum_copy(b).start()

        @pl.when(i == 1)
        def _():
            steps(2, 1, inside, (False,))

        @pl.when(i == 2)
        def _():
            steps(2, 1, inside, (True,))

        @pl.when(i == lines - 1)
        def _():
            steps(2, 1, at_end, (False,))

    for s in PHASES[3]:
        cross_pair(s).start()

    @pl.loop(0, lines)
    def _(i):
        @pl.when(i == 0)
        def _():
            for d in range(2, lines):
                steps(2, d, inside, (False,))
            steps(2, 1, at_end, (True,))

        @pl.when(i == 1)
        def _():
            for d in range(2, lines):
                steps(2, d, inside, (True,))
            for d in range(2, last):
                steps(2, d, at_end, (False,))
            own(3)
            crossed(3)

        @pl.when(i == lines - 2)
        def _():
            for d in range(2, last):
                steps(2, d, at_end, (True,))
            steps(2, last, at_end & (last > 1), (False,))

        @pl.when(i == lines - 1)
        def _():
            steps(3, 1, inside)
            steps(2, last, at_end & (last > 1), (True,))

        k = nth(i)
        here = pl.ds(pl.multiple_of(k * 2 * model, LANES), 2 * model)
        for side in range(2):
            b = 2 * k + side
            sum_copy(b).wait_recv()
            for j in range(2):
                slot = c * 2 + j
                there = slice(side * model, (side + 1) * model)
                base = rows_in[slot, :, here][:, there].astype(F32)
                total = sum_out[b, j].astype(F32) + sum_in[b, j].astype(F32)
                middle[k, slot, :, there] = (base + total).astype(BF16)
        for j in range(2):
            mid_copy(k, c * 2 + j).start()

    def norm_middle(slot):
        @pl.loop(0, rows // tile)
        def _(i):
            here = pl.ds(pl.multiple_of(i * tile, tile), tile)
            wide = [middle[k, slot, here, :].astype(F32) for k in range(lines)]
            total = sum(jnp.sum(w * w, axis=-1, keepdims=True) for w in wide)
            scale = lax.rsqrt(total / depth + 1e-06)
            for k in range(lines):
                there = slice(k * 2 * model, (k + 1) * 2 * model)
                normed[slot, here, there] = (wide[k] * scale * channel_gain[:, there]).astype(BF16)

    steps_from(3, 2, inside)
    for j in range(2):
        norm_middle(c * 2 + j)
    for j in range(2):

        @pl.loop(0, lines)
        def _(k):
            mid_copy(k, peers + j).wait_recv()

        norm_middle(peers + j)

    steps(3, 1, at_end)
    for s in PHASES[2]:
        complete(s)

    def channel(slot):
        both = dot(normed[slot], g34[...].reshape(depth, 2 * units))
        pieces = [(0, main, 0, main)]
        if rest:
            pieces.append((main, units, 2 * main, 2 * main + rest))
        for first, end, gate_at, up_at in pieces:
            size = end - first
            gates = both[:, gate_at : gate_at + size].astype(BF16).astype(F32)
            ups = both[:, up_at : up_at + size].astype(BF16).astype(F32)
            place = lax.broadcasted_iota(jnp.int32, (rows, size), 0) % SEQ_LEN
            conv = taps_here[KCONV - 1 : KCONV, first:end] * gates
            for lag in range(1, KCONV):
                shifted = jnp.where(place >= lag, pltpu.roll(gates, lag, 0), 0.0)
                conv = conv + taps_here[KCONV - 1 - lag : KCONV - lag, first:end] * shifted
            hidden[slot, :, first:end] = (jax.nn.silu(conv) * ups).astype(BF16)

    def half_channel(side):
        @pl.loop(0, 2)
        def _(core):
            channel(core * 2 + side)

    @pl.loop(0, fs)
    def _(b):
        part_copy(b).wait_send()
        sum_copy(b).wait_send()

    def last_part(b, side):
        return remote(
            part_out.at[b, side],
            part_in.at[b, side],
            part_send2.at[b, side],
            part_recv2.at[b, side],
            twin,
        )

    def last_copy(b):
        return remote(sum_out.at[b, 0], last_in.at[b], last_send.at[b], last_recv.at[b], across)

    def of_block(i):
        return 2 * nth(i // 2) + jnp.where(i % 2 == 0, y, 1 - y)

    def give(b, side):
        part_out[b, side] = dot(hidden[peers + side], g5[b]).astype(BF16)
        last_part(b, side).start()

    def give_both(b):
        lhs = hidden[pl.ds(peers, 2)].reshape(2 * rows, units)
        part_out[b] = dot(lhs, g5[b]).reshape(2, rows, model).astype(BF16)
        for side in range(2):
            last_part(b, side).start()

    def send_blocks(first, end, both):
        @pl.loop(first, end + 1)
        def _(i):
            @pl.when(i < end)
            def _():
                b = of_block(i)

                @pl.when(b != f)
                def _():
                    pair_wait(5, b)

                if both:
                    give_both(b)
                else:
                    give(b, 1 - y)

            @pl.when(i > first)
            def _():
                b = of_block(i - 1)
                value = dot(hidden[beside], g5[b])
                last_part(b, 1 - y).wait_recv()
                sum_out[b, 0] = (value + part_in[b, 1 - y].astype(F32)).astype(BF16)
                last_copy(b).start()

    half_channel(1 - y)
    split = lines // 2
    reach = min(lines, max(split, 3))
    for d in range(2, reach):
        steps(3, d, at_end)
    send_blocks(0, 2 * split, False)
    half_channel(y)

    @pl.loop(0, 2 * split)
    def _(i):
        give(of_block(i), y)

    for d in range(reach, lines):
        steps(3, d, at_end)
    send_blocks(2 * split, fs, True)

    def out_copy(k):
        here = pl.ds(pl.multiple_of(k * 2 * model, LANES), 2 * model)
        return pltpu.make_async_copy(out_here.at[k], out.at[:, here], out_sem.at[k])

    @pl.loop(0, lines)
    def _(i):
        k = nth(i)
        values = [dot(hidden[mine], g5[2 * k + side]) for side in range(2)]
        for side in range(2):
            b = 2 * k + side
            last_part(b, y).wait_recv()
            last_copy(b).wait_recv()
            total = values[side] + part_in[b, y].astype(F32) + last_in[b].astype(F32)
            there = slice(side * model, (side + 1) * model)
            total = total + middle[k, mine, :, there].astype(F32)
            out_here[k, :, there] = total.astype(BF16)
        out_copy(k).start()

    for s in range(STREAMS):
        cross_line(s).wait_send()
        if s in BY_COPY:
            to_copy(s, beyond).wait_send()
        else:
            cross_pair(s).wait_send()

        @pl.when(has_left)
        def _():
            for side in range(2):
                on_line(s, 2 * q + side, left_send.at[s, side], left).wait_send()

        @pl.loop(0, fs)
        def _(source):
            k = source // 2

            @pl.when(((k <= q) & has_right) | ((k > q) & has_left))
            def _():
                on_line(s, source, line_send.at[s, source], across).wait_send()

            @pl.when(k != q)
            def _():
                to_copy(s, source).wait_send()

    for copy in (row_to_across, row_to_twin, row_forward, *stat_copies):
        copy.wait_send()

    @pl.loop(0, fs)
    def _(b):
        for side in range(2):
            last_part(b, side).wait_send()
        last_copy(b).wait_send()

    @pl.loop(0, lines)
    def _(k):
        for j in range(2):
            mid_copy(k, c * 2 + j).wait_send()
        out_copy(k).wait()


def body(reps, fs, tps):
    assert reps == 2 and tps == 2 and fs % 2 == 0

    def on_device(
        residual,
        mixer_gain,
        gating_proj,
        spatial_proj,
        spatial_gain,
        spatial_bias,
        spatial_mix,
        spatial_offset,
        mixer_out,
        channel_gain,
        gate_proj,
        up_proj,
        conv_taps,
        down_proj,
    ):
        rows, depth = residual.shape
        assert rows % SEQ_LEN == 0
        own_rows = gating_proj.shape[0]
        width = gating_proj.shape[1] // 2
        units = gate_proj.shape[1] // 2
        group = gating_proj.shape[1] * tps
        columns = mixer_out.shape[1]
        span = spatial_mix.shape[1]
        heads = width // HEAD
        lines = fs // 2
        vmem, hbm = pl.BlockSpec(memory_space=pltpu.VMEM), pl.BlockSpec(memory_space=pl.ANY)
        dma = pltpu.SemaphoreType.DMA
        return pl.pallas_call(
            functools.partial(kernel, (fs, rows, depth, group, width, units)),
            out_shape=jax.ShapeDtypeStruct((rows, depth), BF16),
            in_specs=[hbm] * 8 + [vmem] * 6,
            out_specs=hbm,
            scratch_shapes=[
                pltpu.VMEM((fs, own_rows, width), BF16),
                pltpu.VMEM((fs, own_rows, width), BF16),
                pltpu.VMEM((fs, width, columns), BF16),
                pltpu.VMEM((fs, own_rows, 2 * units), BF16),
                pltpu.VMEM((fs, units, columns), BF16),
                pltpu.VMEM((2, own_rows, 2 * units), BF16),
                pltpu.VMEM((own_rows, 2 * units), BF16),
                pltpu.VMEM((KCONV, units), F32),
                pltpu.VMEM((4, rows, depth), BF16),
                pltpu.VMEM((4, rows, depth), BF16),
                pltpu.VMEM((lines, 4, rows, 2 * columns), BF16),
                pltpu.VMEM((4, rows, width), F32),
                pltpu.VMEM((4, rows, width), F32),
                pltpu.VMEM((4, rows, width), BF16),
                pltpu.VMEM((4, rows, units), BF16),
                pltpu.VMEM((heads, span, span), BF16),
                pltpu.VMEM((heads * HEAD // LANES, span, span * LANES // HEAD), BF16),
                pltpu.VMEM((span, width), F32),
                pltpu.VMEM((4, 2, 4 * rows), F32),
                pltpu.VMEM((fs, 2, rows, columns), BF16),
                pltpu.VMEM((fs, 2, rows, columns), BF16),
                pltpu.VMEM((fs, 2, rows, columns), BF16),
                pltpu.VMEM((fs, 2, rows, columns), BF16),
                pltpu.VMEM((fs, rows, columns), BF16),
                pltpu.VMEM((lines, rows, 2 * columns), BF16),
                dma((STREAMS + 2,)),
                dma((lines,)),
                dma((STREAMS, fs)),
                dma((STREAMS, fs)),
                dma((STREAMS, 2)),
                dma((STREAMS, fs)),
                dma((STREAMS, fs)),
                dma((STREAMS, 2)),
                dma((3,)),
                dma((4,)),
                dma((3,)),
                dma((4,)),
                dma((fs,)),
                dma((fs,)),
                dma((fs,)),
                dma((fs,)),
                dma((lines, 4)),
                dma((lines, 4)),
                dma((fs, 2)),
                dma((fs, 2)),
                dma((fs,)),
                dma((fs,)),
            ],
            compiler_params=pltpu.CompilerParams(
                collective_id=0, has_side_effects=True, vmem_limit_bytes=67043328
            ),
        )(
            residual,
            gating_proj,
            spatial_proj,
            mixer_out,
            gate_proj,
            up_proj,
            down_proj,
            spatial_mix,
            mixer_gain.reshape(1, -1),
            channel_gain.reshape(1, -1),
            spatial_gain.reshape(1, -1),
            spatial_bias.reshape(1, -1),
            spatial_offset,
            conv_taps,
        )

    return on_device


def solution(mesh):
    in_specs = (
        P(("rep", "fs", "tp"), None),
        P(),
        P("fs", "tp"),
        P("fs", "tp"),
        P(),
        P(),
        P(),
        P(),
        P("tp", "fs"),
        P(),
        P("fs", "tp"),
        P("fs", "tp"),
        P(),
        P("tp", "fs"),
    )
    out_specs = P(("rep", "fs", "tp"), None)
    return jax.shard_map(
        body(mesh.shape["rep"], mesh.shape["fs"], mesh.shape["tp"]),
        mesh=mesh,
        in_specs=in_specs,
        out_specs=out_specs,
        check_vma=False,
    )
```

```python
import functools

import jax
import jax.numpy as jnp
from jax import lax
from jax.experimental import pallas as pl
from jax.experimental.pallas import tpu as pltpu
from jax.sharding import PartitionSpec as P

HEAD = 64
SEGMENT = 64
KCONV = 3
SEQ_LEN = 256
LANES = 128

MESH = pl.DeviceIdType.MESH
BF16, F32 = jnp.bfloat16, jnp.float32

PHASES = ((0, 1), (2,), (3, 4), (5,))
STREAMS = 6


def dot(a, b):
    return jnp.dot(a, b, preferred_element_type=F32)


def kernel(
    dims,
    residual,
    gating,
    spatial,
    mixer_out,
    gate,
    up,
    down,
    mix,
    mixer_gain,
    channel_gain,
    spatial_gain,
    spatial_bias,
    offset,
    taps,
    out,
    g0,
    g1,
    g2,
    g34,
    g5,
    raw,
    cross,
    taps_here,
    rows_in,
    normed,
    middle,
    act_u,
    act_v,
    gated,
    hidden,
    mixw,
    wcat,
    offs,
    stat,
    part_out,
    part_in,
    sum_out,
    sum_in,
    last_in,
    out_here,
    local_sem,
    out_sem,
    line_recv,
    pair_each,
    pair_all,
    left_send,
    right_send,
    pair_send,
    cross_send,
    row_send,
    row_recv,
    stat_send,
    stat_recv,
    part_send,
    part_recv,
    sum_send,
    sum_recv,
    mid_send,
    mid_recv,
    part_send2,
    part_recv2,
    last_send,
    last_recv,
):
    fs, rows, depth, group, width, units = dims
    lines = fs // 2
    blocks = (g0, g1, g2, g34, g34, g5)
    halves = [block.shape[1] // 2 for block in blocks]
    sizes = [size // 2 if s in PHASES[2] else size for s, size in enumerate(halves)]
    starts = [sizes[s] if s == PHASES[2][1] else 0 for s in range(STREAMS)]
    r, f, c = lax.axis_index("rep"), lax.axis_index("fs"), lax.axis_index("tp")
    q, y = f // 2, f % 2
    beyond = f + 1 - 2 * y
    mine = c * 2 + y
    beside = c * 2 + 1 - y
    peers = (1 - c) * 2
    left, right = (r, f - 2, c), (r, f + 2, c)
    across, copy_chip = (r, beyond, c), (1 - r, f, c)
    twin, diag = (r, f, 1 - c), (r, beyond, 1 - c)
    has_left, has_right = q > 0, q < lines - 1

    def remote(src, dst, send, recv, device):
        return pltpu.make_async_remote_copy(
            src_ref=src,
            dst_ref=dst,
            send_sem=send,
            recv_sem=recv,
            device_id=device,
            device_id_type=MESH,
        )

    def at(start, size, step):
        return pl.ds(pl.multiple_of(start, step), size)

    own_copies = {
        0: (gating.at[:, at(y * width, width, LANES)], g0.at[f]),
        1: (spatial.at[:, at(y * width, width, LANES)], g1.at[f]),
        2: (mixer_out.at[at(y * width, width, 16)], g2.at[f]),
        3: (gate, raw.at[0]),
        4: (up, raw.at[1]),
        5: (down.at[at(y * units, units, 16)], g5.at[f]),
    }
    own_copies = [
        pltpu.make_async_copy(*own_copies[s], local_sem.at[s]) for s in range(STREAMS)
    ]
    heads = mixw.shape[0]
    head = mine * heads
    row_copy = pltpu.make_async_copy(residual, rows_in.at[mine], local_sem.at[STREAMS])
    mix_copy = pltpu.make_async_copy(mix.at[pl.ds(head, heads)], mixw, local_sem.at[STREAMS + 1])
    for copy in own_copies[:2] + [row_copy] + own_copies[2:] + [mix_copy]:
        copy.start()

    barrier = pltpu.get_barrier_semaphore()
    for device in (across, copy_chip, twin, diag):
        pl.semaphore_signal(barrier, inc=1, device_id=device, device_id_type=MESH)

    @pl.when(has_left)
    def _():
        pl.semaphore_signal(barrier, inc=1, device_id=left, device_id_type=MESH)

    @pl.when(has_right)
    def _():
        pl.semaphore_signal(barrier, inc=1, device_id=right, device_id_type=MESH)

    pl.semaphore_wait(barrier, 4 + jnp.minimum(q, 1) + jnp.minimum(lines - 1 - q, 1))

    def half(s, source, h):
        return blocks[s].at[source, at(h * halves[s] + starts[s], sizes[s], 16)]

    def on_line(s, source, send, device):
        ref = half(s, source, r)
        return remote(ref, ref, send, line_recv.at[s, source], device)

    def pair_sem(s, source):
        each = PHASES[1] + PHASES[3]
        return pair_each.at[each.index(s), source] if s in each else pair_all.at[s]

    def to_copy(s, source):
        ref = half(s, source, r)
        return remote(ref, ref, pair_send.at[s], pair_sem(s, source), copy_chip)

    def line_wait(s, source):
        on_line(s, source, left_send.at[s], across).wait_recv()

    def pair_wait(s, source):
        ref = half(s, source, 1 - r)
        remote(ref, ref, pair_send.at[s], pair_sem(s, source), copy_chip).wait_recv()

    def bulk(ref, sem):
        return remote(ref, ref, sem, sem, across)

    def chunks(s, count, sem):
        return bulk(blocks[s].at[pl.ds(0, count), pl.ds(0, sizes[s])], sem)

    def crossing(s, h):
        start = (1 - y) * width
        here = at(h * halves[s], halves[s], 16)
        if s < 2:
            src = (gating, spatial)[s].at[here, at(start, width, LANES)]
        elif s == 2:
            src = mixer_out.at[at(start + h * halves[s], halves[s], 16)]
        elif s < 5:
            src = cross.at[at(h * halves[s] + starts[s], sizes[s], 16)]
        else:
            src = down.at[at((1 - y) * units + h * halves[s], halves[s], 16)]
        return src, half(s, f, h)

    def cross_line(s):
        src, dst = crossing(s, r)
        return remote(src, dst, cross_send.at[s], line_recv.at[s, f], across)

    def cross_pair(s):
        src, dst = crossing(s, 1 - r)
        return remote(src, dst, cross_send.at[s], pair_sem(s, f), across)

    def both_ways(s, source):
        @pl.when(has_left)
        def _():
            on_line(s, source, left_send.at[s], left).start()

        @pl.when(has_right)
        def _():
            on_line(s, source, right_send.at[s], right).start()

    def own(p):
        for s in PHASES[p]:
            both_ways(s, f)

    def crossed(p, only=None):
        for s in PHASES[p] if only is None else (only,):
            line_wait(s, beyond)
            both_ways(s, beyond)

    near = jnp.minimum(q, lines - 1 - q)
    at_end, inside = near == 0, near > 0

    def step(s, d, other, who):
        @pl.when((q - d >= 0) & who)
        def _():
            source = (beyond if other else f) - 2 * d
            line_wait(s, source)

            @pl.when(has_right)
            def _():
                on_line(s, source, right_send.at[s], right).start()

            to_copy(s, source).start()

        @pl.when((q + d < lines) & who)
        def _():
            source = (beyond if other else f) + 2 * d
            line_wait(s, source)

            @pl.when(has_left)
            def _():
                on_line(s, source, left_send.at[s], left).start()

            to_copy(s, source).start()

    def steps(p, d, who=True, others=(False, True)):
        for other in others:
            for s in PHASES[p]:
                step(s, d, other, who)

    def steps_from(p, first, who):
        for d in range(first, lines):
            steps(p, d, who)

    def complete(s):
        chunks(s, fs - 1, pair_all.at[s]).wait_recv()

    row_to_across = remote(residual, rows_in.at[mine], row_send, row_recv.at[mine], across)
    row_to_twin = remote(residual, rows_in.at[mine], row_send, row_recv.at[mine], twin)
    for s in PHASES[0] + PHASES[1]:
        cross_line(s).start()
    row_to_across.start()
    row_to_twin.start()
    for s in PHASES[0]:
        cross_pair(s).start()
        own_copies[s].wait()
    own(0)

    def row_wait(slot):
        remote(
            rows_in.at[slot], rows_in.at[slot], row_send, row_recv.at[slot], across
        ).wait_recv()

    tile = 64

    def norm_in(slot):
        @pl.loop(0, rows // tile)
        def _(i):
            here = pl.ds(pl.multiple_of(i * tile, tile), tile)
            wide = rows_in[slot, here, :].astype(F32)
            scale = lax.rsqrt(jnp.mean(wide * wide, axis=-1, keepdims=True) + 1e-06)
            normed[slot, here, :] = (wide * scale * mixer_gain[...]).astype(BF16)

    main = units // LANES * LANES
    rest = units - main
    for s in PHASES[2]:
        own_copies[s].wait()
    for way in range(2):

        @pl.when(y == way)
        def _():
            for i in range(2):
                for ref, first in ((g34.at[f], way * units), (cross, (1 - way) * units)):
                    ref[:, i * main : (i + 1) * main] = raw[i, :, first : first + main]
                    if rest:
                        there = slice(2 * main + i * rest, 2 * main + (i + 1) * rest)
                        ref[:, there] = raw[i, :, first + main : first + units]

    for k in range(4):

        @pl.when(mine == k)
        def _():
            taps_here[...] = taps[:, k * units : (k + 1) * units]

    row_copy.wait()
    norm_in(mine)
    own_copies[2].wait()
    own_copies[5].wait()
    mix_copy.wait()

    for s in PHASES[0]:
        step(s, 1, False, True)
        crossed(0, s)
    for d in range(1, lines - 1):
        for s in PHASES[0]:
            step(s, d + 1, False, True)
            step(s, d, True, True)
    own(1)
    crossed(1)
    for s in PHASES[2]:
        cross_line(s).start()
    steps(0, lines - 1, True, (True,))
    row_wait(beside)
    row_forward = remote(
        rows_in.at[beside], rows_in.at[beside], row_send, row_recv.at[beside], twin
    )
    row_forward.start()
    norm_in(beside)
    for s in PHASES[1]:
        cross_pair(s).start()
    steps(1, 1, inside)
    for j in range(2):
        row_wait(peers + j)
        norm_in(peers + j)
    steps_from(1, 2, inside)
    own(2)
    steps(1, 1, at_end)

    span = mixw.shape[1]
    per = LANES // HEAD
    at_row = lax.broadcasted_iota(jnp.int32, (span, span), 0)
    at_col = lax.broadcasted_iota(jnp.int32, (span, span), 1)
    allowed = at_col // SEGMENT <= at_row // SEGMENT
    eye = at_col == at_row
    lane = lax.broadcasted_iota(jnp.int32, (span, LANES), 1)

    def column_of(row):
        return jnp.sum(
            jnp.where(eye, jnp.broadcast_to(row, (span, span)), 0.0), axis=1, keepdims=True
        )

    def row_of(column):
        return jnp.sum(
            jnp.where(eye, jnp.broadcast_to(column, (span, span)), 0.0), axis=0, keepdims=True
        )

    for p in range(heads // per):
        off = jnp.zeros((span, LANES), F32)
        for k in range(per):
            h = p * per + k
            wcat[p, :, k * span : (k + 1) * span] = jnp.where(
                allowed, mixw[h].astype(F32), 0.0
            ).astype(BF16)
            here = column_of(offset[pl.ds(head + h, 1), :])
            off = jnp.where(lane // HEAD == k, here, off)
        offs[:, p * LANES : (p + 1) * LANES] = off

    for s in PHASES[0]:
        complete(s)

    def project_v(slot):
        v = dot(normed[slot], g1[...].reshape(depth, width)).astype(BF16).astype(F32)
        v = jax.nn.gelu(v)
        act_v[slot] = v
        total = jnp.sum(v, axis=-1, keepdims=True)
        squares = jnp.sum(v * v, axis=-1, keepdims=True)
        for b in range(rows // span):
            here = pl.ds(pl.multiple_of(slot * rows + b * span, LANES), span)
            stat[mine, 0:1, here] = row_of(total[b * span : (b + 1) * span])
            stat[mine, 1:2, here] = row_of(squares[b * span : (b + 1) * span])

    def project_u(slot):
        u = dot(normed[slot], g0[...].reshape(depth, width)).astype(BF16).astype(F32)
        act_u[slot] = jax.nn.gelu(u)

    last = lines - 1

    @pl.loop(0, 4)
    def _(slot):
        project_v(slot)

        @pl.when(slot == 3)
        def _():
            crossed(2)
            for d in range(2, last):
                steps(1, d, at_end, (False,))

    for device in (across, twin, diag):
        remote(stat.at[mine], stat.at[mine], stat_send, stat_recv.at[mine], device).start()
    cross_pair(PHASES[2][0]).start()

    @pl.loop(0, 4)
    def _(slot):
        project_u(slot)

        @pl.when(slot == 1)
        def _():
            for d in range(2, last):
                steps(1, d, at_end, (True,))

    for s in PHASES[3]:
        cross_line(s).start()
    for other in (beside, peers, peers + 1):
        remote(
            stat.at[other], stat.at[other], stat_send, stat_recv.at[other], across
        ).wait_recv()

    gain_here = spatial_gain[:, pl.ds(pl.multiple_of(mine * width, LANES), width)]
    bias_here = spatial_bias[:, pl.ds(pl.multiple_of(mine * width, LANES), width)]
    pairs = heads // per

    def gate_slot(slot):
        low = []
        for b in range(rows // span):
            here = pl.ds(pl.multiple_of(slot * rows + b * span, LANES), span)
            sums = stat[0, :, here] + stat[1, :, here] + stat[2, :, here] + stat[3, :, here]
            mean_row = sums[0:1] / group
            var_row = sums[1:2] / group - mean_row * mean_row
            mean = column_of(mean_row)
            scale = lax.rsqrt(column_of(var_row) + 1e-05)
            v = act_v[slot, b * span : (b + 1) * span, :]
            vnorm = (v - mean) * scale * gain_here + bias_here
            parts = []
            for p in range(pairs):
                tile_v = vnorm[:, p * LANES : (p + 1) * LANES]
                parts.append(
                    jnp.concatenate(
                        [
                            jnp.where(lane // HEAD == k, tile_v, 0.0).astype(BF16)
                            for k in range(per)
                        ],
                        axis=0,
                    )
                )
            low.append(parts)
        for p in range(pairs):
            rhs = jnp.concatenate([parts[p] for parts in low], axis=1)
            mixed = dot(wcat[p], rhs)
            here = slice(p * LANES, (p + 1) * LANES)
            for b in range(rows // span):
                there = slice(b * span, (b + 1) * span)
                m = mixed[:, b * LANES : (b + 1) * LANES] + offs[:, here]
                gated[slot, there, here] = (act_u[slot, there, here] * m).astype(BF16)

    @pl.loop(0, 4)
    def _(slot):
        gate_slot(slot)

    model = g2.shape[2]
    def nth(i):
        d = (i + 1) // 2
        close = jnp.where(i % 2 == 1, q + d, q - d)
        far = jnp.where(q < lines - 1 - q, i, lines - 1 - i)
        return jnp.where(i <= 2 * near, close, far)

    def of_block(i):
        return 2 * nth(i // 2) + jnp.where(i % 2 == 0, y, 1 - y)

    def part_copy(b):
        return remote(part_out.at[b], part_in.at[b], part_send, part_recv.at[b], twin)

    def sum_copy(b):
        return remote(sum_out.at[b], sum_in.at[b], sum_send, sum_recv.at[b], across)

    def mid_copy(k, slot):
        return remote(
            middle.at[k, slot], middle.at[k, slot], mid_send, mid_recv.at[slot], twin
        )

    def mixer_product(first, b):
        lhs = gated[pl.ds(first, 2)].reshape(2 * rows, width)
        return dot(lhs, g2[b]).reshape(2, rows, model)

    @pl.loop(0, fs + 1)
    def _(i):
        @pl.when(i < fs)
        def _():
            b = of_block(i)

            @pl.when(b != f)
            def _():
                pair_wait(2, b)

            part_out[b] = mixer_product(peers, b).astype(BF16)
            part_copy(b).start()

        @pl.when(i > 0)
        def _():
            b = of_block(i - 1)
            value = mixer_product(c * 2, b)
            part_copy(b).wait_recv()
            sum_out[b] = (value + part_in[b].astype(F32)).astype(BF16)
            sum_copy(b).start()

        @pl.when(i == 1)
        def _():
            steps(1, last, at_end & (last > 1))

        @pl.when(i == 3)
        def _():
            steps(2, 1, inside, (False,))

        @pl.when(i == 5)
        def _():
            steps(2, 1, inside, (True,))

        @pl.when(i == fs // 2)
        def _():
            step(PHASES[2][0], 1, False, at_end)

        @pl.when(i == fs - 1)
        def _():
            step(PHASES[2][1], 1, False, at_end)

    for s in PHASES[2][1:] + PHASES[3]:
        cross_pair(s).start()

    @pl.loop(0, lines)
    def _(i):
        @pl.when(i == 0)
        def _():
            for d in range(2, lines):
                steps(2, d, inside, (False,))
            steps(2, 1, at_end, (True,))

        @pl.when(i == 1)
        def _():
            for d in range(2, lines):
                steps(2, d, inside, (True,))
            for d in range(2, last):
                steps(2, d, at_end, (False,))
            own(3)
            crossed(3)

        @pl.when(i == lines - 2)
        def _():
            for d in range(2, last):
                steps(2, d, at_end, (True,))
            steps(2, last, at_end & (last > 1), (False,))

        @pl.when(i == lines - 1)
        def _():
            steps(3, 1, inside)
            steps(2, last, at_end & (last > 1), (True,))

        k = nth(i)
        here = pl.ds(pl.multiple_of(k * 2 * model, LANES), 2 * model)
        for side in range(2):
            b = 2 * k + side
            sum_copy(b).wait_recv()
            for j in range(2):
                slot = c * 2 + j
                there = slice(side * model, (side + 1) * model)
                base = rows_in[slot, :, here][:, there].astype(F32)
                total = sum_out[b, j].astype(F32) + sum_in[b, j].astype(F32)
                middle[k, slot, :, there] = (base + total).astype(BF16)
        for j in range(2):
            mid_copy(k, c * 2 + j).start()

    def norm_middle(slot):
        @pl.loop(0, rows // tile)
        def _(i):
            here = pl.ds(pl.multiple_of(i * tile, tile), tile)
            wide = [middle[k, slot, here, :].astype(F32) for k in range(lines)]
            total = sum(jnp.sum(w * w, axis=-1, keepdims=True) for w in wide)
            scale = lax.rsqrt(total / depth + 1e-06)
            for k in range(lines):
                there = slice(k * 2 * model, (k + 1) * 2 * model)
                normed[slot, here, there] = (wide[k] * scale * channel_gain[:, there]).astype(BF16)

    steps_from(3, 2, inside)
    for j in range(2):
        norm_middle(c * 2 + j)
    for j in range(2):
        bulk(middle.at[:, peers + j], mid_recv.at[peers + j]).wait_recv()
        norm_middle(peers + j)

    steps(3, 1, at_end)
    for s in PHASES[2]:
        complete(s)

    def channel(slot):
        both = dot(normed[slot], g34[...].reshape(depth, 2 * units))
        pieces = [(0, main, 0, main)]
        if rest:
            pieces.append((main, units, 2 * main, 2 * main + rest))
        for first, end, gate_at, up_at in pieces:
            size = end - first
            gates = both[:, gate_at : gate_at + size].astype(BF16).astype(F32)
            ups = both[:, up_at : up_at + size].astype(BF16).astype(F32)
            place = lax.broadcasted_iota(jnp.int32, (rows, size), 0) % SEQ_LEN
            conv = taps_here[KCONV - 1 : KCONV, first:end] * gates
            for lag in range(1, KCONV):
                shifted = jnp.where(place >= lag, pltpu.roll(gates, lag, 0), 0.0)
                conv = conv + taps_here[KCONV - 1 - lag : KCONV - lag, first:end] * shifted
            hidden[slot, :, first:end] = (jax.nn.silu(conv) * ups).astype(BF16)

    bulk(part_out, part_send).wait_send()
    bulk(sum_out, sum_send).wait_send()

    def last_part(b, side):
        return remote(
            part_out.at[b, side],
            part_in.at[b, side],
            part_send2,
            part_recv2.at[b, side],
            twin,
        )

    def last_copy(b):
        return remote(sum_out.at[b, 0], last_in.at[b], last_send, last_recv.at[b], across)

    def give(b, side):
        part_out[b, side] = dot(hidden[peers + side], g5[b]).astype(BF16)
        last_part(b, side).start()

    def give_both(b):
        lhs = hidden[pl.ds(peers, 2)].reshape(2 * rows, units)
        part_out[b] = dot(lhs, g5[b]).reshape(2, rows, model).astype(BF16)
        for side in range(2):
            last_part(b, side).start()

    def pass_on(b):
        value = dot(hidden[beside], g5[b])
        last_part(b, 1 - y).wait_recv()
        sum_out[b, 0] = (value + part_in[b, 1 - y].astype(F32)).astype(BF16)
        last_copy(b).start()

    def send_blocks(first, end):
        @pl.loop(first, end)
        def _(i):
            b = of_block(i)
            pair_wait(5, b)
            give_both(b)
            pass_on(b)

    most = (last,) if last > 1 else ()
    channel(1 - y)

    @pl.when(c == 1)
    def _():
        give(f, 1 - y)

    @pl.when(c == 0)
    def _():
        pass_on(f)

    for d in range(2, last):
        steps(3, d, at_end, (False,))
    channel(3 - y)

    @pl.when(c == 0)
    def _():
        give(f, 1 - y)

    pair_wait(5, beyond)
    give(beyond, 1 - y)

    @pl.when(c == 1)
    def _():
        pass_on(f)

    pass_on(beyond)
    for d in range(2, last):
        steps(3, d, at_end, (True,))

    @pl.loop(0, 2)
    def _(core):
        channel(core * 2 + y)

    for d in most:
        steps(3, d, at_end, (False,))
    give(f, y)
    give(beyond, y)
    split = lines // 2
    if split > 1:
        send_blocks(2, 2 * split)
    for d in most:
        steps(3, d, at_end, (True,))
    send_blocks(2 * split, fs)

    def out_copy(k):
        here = pl.ds(pl.multiple_of(k * 2 * model, LANES), 2 * model)
        return pltpu.make_async_copy(out_here.at[k], out.at[:, here], out_sem.at[k])

    @pl.loop(0, lines)
    def _(i):
        k = nth(i)
        values = [dot(hidden[mine], g5[2 * k + side]) for side in range(2)]
        for side in range(2):
            b = 2 * k + side
            last_part(b, y).wait_recv()
            last_copy(b).wait_recv()
            total = values[side] + part_in[b, y].astype(F32) + last_in[b].astype(F32)
            there = slice(side * model, (side + 1) * model)
            total = total + middle[k, mine, :, there].astype(F32)
            out_here[k, :, there] = total.astype(BF16)
        out_copy(k).start()

    for s in range(STREAMS):
        chunks(s, 2, cross_send.at[s]).wait_send()
        chunks(s, fs - 2, pair_send.at[s]).wait_send()
    for k in range(lines):

        @pl.when(q == k)
        def _():
            for s in range(STREAMS):
                if k > 0:
                    chunks(s, 2 * (lines - k), left_send.at[s]).wait_send()
                if k < lines - 1:
                    chunks(s, 2 * (k + 1), right_send.at[s]).wait_send()

    bulk(rows_in.at[pl.ds(0, 3)], row_send).wait_send()
    bulk(stat.at[pl.ds(0, 3)], stat_send).wait_send()
    bulk(middle.at[:, pl.ds(0, 2)], mid_send).wait_send()
    bulk(part_out, part_send2).wait_send()
    bulk(last_in, last_send).wait_send()

    @pl.loop(0, lines)
    def _(k):
        out_copy(k).wait()


def body(reps, fs, tps):
    assert reps == 2 and tps == 2 and fs % 2 == 0

    def on_device(
        residual,
        mixer_gain,
        gating_proj,
        spatial_proj,
        spatial_gain,
        spatial_bias,
        spatial_mix,
        spatial_offset,
        mixer_out,
        channel_gain,
        gate_proj,
        up_proj,
        conv_taps,
        down_proj,
    ):
        rows, depth = residual.shape
        assert rows % SEQ_LEN == 0
        own_rows = gating_proj.shape[0]
        width = gating_proj.shape[1] // 2
        units = gate_proj.shape[1] // 2
        group = gating_proj.shape[1] * tps
        columns = mixer_out.shape[1]
        span = spatial_mix.shape[1]
        heads = width // HEAD
        lines = fs // 2
        vmem, hbm = pl.BlockSpec(memory_space=pltpu.VMEM), pl.BlockSpec(memory_space=pl.ANY)
        dma = pltpu.SemaphoreType.DMA
        return pl.pallas_call(
            functools.partial(kernel, (fs, rows, depth, group, width, units)),
            out_shape=jax.ShapeDtypeStruct((rows, depth), BF16),
            in_specs=[hbm] * 8 + [vmem] * 6,
            out_specs=hbm,
            scratch_shapes=[
                pltpu.VMEM((fs, own_rows, width), BF16),
                pltpu.VMEM((fs, own_rows, width), BF16),
                pltpu.VMEM((fs, width, columns), BF16),
                pltpu.VMEM((fs, own_rows, 2 * units), BF16),
                pltpu.VMEM((fs, units, columns), BF16),
                pltpu.VMEM((2, own_rows, 2 * units), BF16),
                pltpu.VMEM((own_rows, 2 * units), BF16),
                pltpu.VMEM((KCONV, units), F32),
                pltpu.VMEM((4, rows, depth), BF16),
                pltpu.VMEM((4, rows, depth), BF16),
                pltpu.VMEM((lines, 4, rows, 2 * columns), BF16),
                pltpu.VMEM((4, rows, width), F32),
                pltpu.VMEM((4, rows, width), F32),
                pltpu.VMEM((4, rows, width), BF16),
                pltpu.VMEM((4, rows, units), BF16),
                pltpu.VMEM((heads, span, span), BF16),
                pltpu.VMEM((heads * HEAD // LANES, span, span * LANES // HEAD), BF16),
                pltpu.VMEM((span, width), F32),
                pltpu.VMEM((4, 2, 4 * rows), F32),
                pltpu.VMEM((fs, 2, rows, columns), BF16),
                pltpu.VMEM((fs, 2, rows, columns), BF16),
                pltpu.VMEM((fs, 2, rows, columns), BF16),
                pltpu.VMEM((fs, 2, rows, columns), BF16),
                pltpu.VMEM((fs, rows, columns), BF16),
                pltpu.VMEM((lines, rows, 2 * columns), BF16),
                dma((STREAMS + 2,)),
                dma((lines,)),
                dma((STREAMS, fs)),
                dma((2, fs)),
                dma((STREAMS,)),
                dma((STREAMS,)),
                dma((STREAMS,)),
                dma((STREAMS,)),
                dma((STREAMS,)),
                dma(()),
                dma((4,)),
                dma(()),
                dma((4,)),
                dma(()),
                dma((fs,)),
                dma(()),
                dma((fs,)),
                dma(()),
                dma((4,)),
                dma(()),
                dma((fs, 2)),
                dma(()),
                dma((fs,)),
            ],
            compiler_params=pltpu.CompilerParams(
                collective_id=0, has_side_effects=True, vmem_limit_bytes=67043328
            ),
        )(
            residual,
            gating_proj,
            spatial_proj,
            mixer_out,
            gate_proj,
            up_proj,
            down_proj,
            spatial_mix,
            mixer_gain.reshape(1, -1),
            channel_gain.reshape(1, -1),
            spatial_gain.reshape(1, -1),
            spatial_bias.reshape(1, -1),
            spatial_offset,
            conv_taps,
        )

    return on_device


def solution(mesh):
    in_specs = (
        P(("rep", "fs", "tp"), None),
        P(),
        P("fs", "tp"),
        P("fs", "tp"),
        P(),
        P(),
        P(),
        P(),
        P("tp", "fs"),
        P(),
        P("fs", "tp"),
        P("fs", "tp"),
        P(),
        P("tp", "fs"),
    )
    out_specs = P(("rep", "fs", "tp"), None)
    return jax.shard_map(
        body(mesh.shape["rep"], mesh.shape["fs"], mesh.shape["tp"]),
        mesh=mesh,
        in_specs=in_specs,
        out_specs=out_specs,
        check_vma=False,
    )
```

```python
import functools

import jax
import jax.numpy as jnp
from jax import lax
from jax.experimental import pallas as pl
from jax.experimental.pallas import tpu as pltpu
from jax.sharding import PartitionSpec as P

HEAD = 64
SEGMENT = 64
KCONV = 3
SEQ_LEN = 256
LANES = 128

MESH = pl.DeviceIdType.MESH
BF16, F32 = jnp.bfloat16, jnp.float32

PHASES = ((0, 1), (2,), (3, 4), (5,))
STREAMS = 6


def dot(a, b):
    return jnp.dot(a, b, preferred_element_type=F32)


def kernel(
    dims,
    residual,
    gating,
    spatial,
    mixer_out,
    gate,
    up,
    down,
    mix,
    mixer_gain,
    channel_gain,
    spatial_gain,
    spatial_bias,
    offset,
    taps,
    out,
    g0,
    g1,
    g2,
    g34,
    g5,
    raw,
    cross,
    taps_here,
    rows_in,
    normed,
    middle,
    act_u,
    act_v,
    gated,
    hidden,
    mixw,
    wcat,
    offs,
    stat,
    part_out,
    part_in,
    sum_out,
    sum_in,
    last_in,
    out_here,
    local_sem,
    out_sem,
    line_recv,
    pair_each,
    pair_all,
    left_send,
    right_send,
    pair_send,
    cross_send,
    row_send,
    row_recv,
    stat_send,
    stat_recv,
    part_send,
    part_recv,
    sum_send,
    sum_recv,
    mid_send,
    mid_recv,
    part_send2,
    part_recv2,
    last_send,
    last_recv,
):
    fs, rows, depth, group, width, units = dims
    lines = fs // 2
    blocks = (g0, g1, g2, g34, g34, g5)
    halves = [block.shape[1] // 2 for block in blocks]
    sizes = [size // 2 if s in PHASES[2] else size for s, size in enumerate(halves)]
    starts = [sizes[s] if s == PHASES[2][1] else 0 for s in range(STREAMS)]
    r, f, c = lax.axis_index("rep"), lax.axis_index("fs"), lax.axis_index("tp")
    q, y = f // 2, f % 2
    beyond = f + 1 - 2 * y
    mine = c * 2 + y
    beside = c * 2 + 1 - y
    peers = (1 - c) * 2
    left, right = (r, f - 2, c), (r, f + 2, c)
    across, copy_chip = (r, beyond, c), (1 - r, f, c)
    twin, diag = (r, f, 1 - c), (r, beyond, 1 - c)
    has_left, has_right = q > 0, q < lines - 1

    def remote(src, dst, send, recv, device):
        return pltpu.make_async_remote_copy(
            src_ref=src,
            dst_ref=dst,
            send_sem=send,
            recv_sem=recv,
            device_id=device,
            device_id_type=MESH,
        )

    def at(start, size, step):
        return pl.ds(pl.multiple_of(start, step), size)

    own_copies = {
        0: (gating.at[:, at(y * width, width, LANES)], g0.at[f]),
        1: (spatial.at[:, at(y * width, width, LANES)], g1.at[f]),
        2: (mixer_out.at[at(y * width, width, 16)], g2.at[f]),
        3: (gate, raw.at[0]),
        4: (up, raw.at[1]),
        5: (down.at[at(y * units, units, 16)], g5.at[f]),
    }
    own_copies = [
        pltpu.make_async_copy(*own_copies[s], local_sem.at[s]) for s in range(STREAMS)
    ]
    heads = mixw.shape[0]
    head = mine * heads
    row_copy = pltpu.make_async_copy(residual, rows_in.at[mine], local_sem.at[STREAMS])
    mix_copy = pltpu.make_async_copy(mix.at[pl.ds(head, heads)], mixw, local_sem.at[STREAMS + 1])
    for copy in own_copies[:2] + [row_copy] + own_copies[2:] + [mix_copy]:
        copy.start()

    barrier = pltpu.get_barrier_semaphore()
    for device in (across, copy_chip, twin, diag):
        pl.semaphore_signal(barrier, inc=1, device_id=device, device_id_type=MESH)

    @pl.when(has_left)
    def _():
        pl.semaphore_signal(barrier, inc=1, device_id=left, device_id_type=MESH)

    @pl.when(has_right)
    def _():
        pl.semaphore_signal(barrier, inc=1, device_id=right, device_id_type=MESH)

    pl.semaphore_wait(barrier, 4 + jnp.minimum(q, 1) + jnp.minimum(lines - 1 - q, 1))

    def half(s, source, h):
        return blocks[s].at[source, at(h * halves[s] + starts[s], sizes[s], 16)]

    def on_line(s, source, send, device):
        ref = half(s, source, r)
        return remote(ref, ref, send, line_recv.at[s, source], device)

    def pair_sem(s, source):
        each = PHASES[1] + PHASES[3]
        return pair_each.at[each.index(s), source] if s in each else pair_all.at[s]

    def to_copy(s, source):
        ref = half(s, source, r)
        return remote(ref, ref, pair_send.at[s], pair_sem(s, source), copy_chip)

    def line_wait(s, source):
        on_line(s, source, left_send.at[s], across).wait_recv()

    def pair_wait(s, source):
        ref = half(s, source, 1 - r)
        remote(ref, ref, pair_send.at[s], pair_sem(s, source), copy_chip).wait_recv()

    def bulk(ref, sem):
        return remote(ref, ref, sem, sem, across)

    def chunks(s, count, sem):
        return bulk(blocks[s].at[pl.ds(0, count), pl.ds(0, sizes[s])], sem)

    def crossing(s, h):
        start = (1 - y) * width
        here = at(h * halves[s], halves[s], 16)
        if s < 2:
            src = (gating, spatial)[s].at[here, at(start, width, LANES)]
        elif s == 2:
            src = mixer_out.at[at(start + h * halves[s], halves[s], 16)]
        elif s < 5:
            src = cross.at[at(h * halves[s] + starts[s], sizes[s], 16)]
        else:
            src = down.at[at((1 - y) * units + h * halves[s], halves[s], 16)]
        return src, half(s, f, h)

    def cross_line(s):
        src, dst = crossing(s, r)
        return remote(src, dst, cross_send.at[s], line_recv.at[s, f], across)

    def cross_pair(s):
        src, dst = crossing(s, 1 - r)
        return remote(src, dst, cross_send.at[s], pair_sem(s, f), across)

    def both_ways(s, source):
        @pl.when(has_left)
        def _():
            on_line(s, source, left_send.at[s], left).start()

        @pl.when(has_right)
        def _():
            on_line(s, source, right_send.at[s], right).start()

    def own(p):
        for s in PHASES[p]:
            both_ways(s, f)

    def crossed(p, only=None):
        for s in PHASES[p] if only is None else (only,):
            line_wait(s, beyond)
            both_ways(s, beyond)

    near = jnp.minimum(q, lines - 1 - q)
    at_end, inside = near == 0, near > 0

    def from_left(s, d, other, who):
        @pl.when((q - d >= 0) & who)
        def _():
            source = (beyond if other else f) - 2 * d
            line_wait(s, source)

            @pl.when(has_right)
            def _():
                on_line(s, source, right_send.at[s], right).start()

            to_copy(s, source).start()

    def from_right(s, d, other, who):
        @pl.when((q + d < lines) & who)
        def _():
            source = (beyond if other else f) + 2 * d
            line_wait(s, source)

            @pl.when(has_left)
            def _():
                on_line(s, source, left_send.at[s], left).start()

            to_copy(s, source).start()

    def step(s, d, other, who):
        from_left(s, d, other, who)
        from_right(s, d, other, who)

    def steps(p, d, who=True, others=(False, True)):
        for other in others:
            for s in PHASES[p]:
                step(s, d, other, who)

    def steps_from(p, first, who):
        for d in range(first, lines):
            steps(p, d, who)

    def complete(s):
        chunks(s, fs - 1, pair_all.at[s]).wait_recv()

    row_to_across = remote(residual, rows_in.at[mine], row_send, row_recv.at[mine], across)
    row_to_twin = remote(residual, rows_in.at[mine], row_send, row_recv.at[mine], twin)
    for s in PHASES[0] + PHASES[1]:
        cross_line(s).start()
    row_to_across.start()
    row_to_twin.start()
    for s in PHASES[0]:
        cross_pair(s).start()
        own_copies[s].wait()
    own(0)

    def row_wait(slot):
        remote(
            rows_in.at[slot], rows_in.at[slot], row_send, row_recv.at[slot], across
        ).wait_recv()

    tile = 64

    def norm_in(slot):
        @pl.loop(0, rows // tile)
        def _(i):
            here = pl.ds(pl.multiple_of(i * tile, tile), tile)
            wide = rows_in[slot, here, :].astype(F32)
            scale = lax.rsqrt(jnp.mean(wide * wide, axis=-1, keepdims=True) + 1e-06)
            normed[slot, here, :] = (wide * scale * mixer_gain[...]).astype(BF16)

    main = units // LANES * LANES
    rest = units - main
    for s in PHASES[2]:
        own_copies[s].wait()
    for way in range(2):

        @pl.when(y == way)
        def _():
            for i in range(2):
                for ref, first in ((g34.at[f], way * units), (cross, (1 - way) * units)):
                    ref[:, i * main : (i + 1) * main] = raw[i, :, first : first + main]
                    if rest:
                        there = slice(2 * main + i * rest, 2 * main + (i + 1) * rest)
                        ref[:, there] = raw[i, :, first + main : first + units]

    for k in range(4):

        @pl.when(mine == k)
        def _():
            taps_here[...] = taps[:, k * units : (k + 1) * units]

    row_copy.wait()
    norm_in(mine)
    own_copies[2].wait()
    own_copies[5].wait()
    mix_copy.wait()

    for s in PHASES[0]:
        step(s, 1, False, True)
        crossed(0, s)
    for d in range(1, lines - 1):
        for s in PHASES[0]:
            step(s, d + 1, False, True)
            step(s, d, True, True)
    own(1)
    crossed(1)
    for s in PHASES[2]:
        cross_line(s).start()
    steps(0, lines - 1, True, (True,))
    row_wait(beside)
    row_forward = remote(
        rows_in.at[beside], rows_in.at[beside], row_send, row_recv.at[beside], twin
    )
    row_forward.start()
    norm_in(beside)
    for s in PHASES[1]:
        cross_pair(s).start()
    steps(1, 1, inside)
    for j in range(2):
        row_wait(peers + j)
        norm_in(peers + j)
    steps_from(1, 2, inside)
    own(2)
    steps(1, 1, at_end)

    span = mixw.shape[1]
    per = LANES // HEAD
    at_row = lax.broadcasted_iota(jnp.int32, (span, span), 0)
    at_col = lax.broadcasted_iota(jnp.int32, (span, span), 1)
    allowed = at_col // SEGMENT <= at_row // SEGMENT
    eye = at_col == at_row
    lane = lax.broadcasted_iota(jnp.int32, (span, LANES), 1)

    def column_of(row):
        return jnp.sum(
            jnp.where(eye, jnp.broadcast_to(row, (span, span)), 0.0), axis=1, keepdims=True
        )

    def row_of(column):
        return jnp.sum(
            jnp.where(eye, jnp.broadcast_to(column, (span, span)), 0.0), axis=0, keepdims=True
        )

    for p in range(heads // per):
        off = jnp.zeros((span, LANES), F32)
        for k in range(per):
            h = p * per + k
            wcat[p, :, k * span : (k + 1) * span] = jnp.where(
                allowed, mixw[h].astype(F32), 0.0
            ).astype(BF16)
            here = column_of(offset[pl.ds(head + h, 1), :])
            off = jnp.where(lane // HEAD == k, here, off)
        offs[:, p * LANES : (p + 1) * LANES] = off

    for s in PHASES[0]:
        complete(s)

    def project_v(slot):
        v = dot(normed[slot], g1[...].reshape(depth, width)).astype(BF16).astype(F32)
        v = jax.nn.gelu(v)
        act_v[slot] = v
        total = jnp.sum(v, axis=-1, keepdims=True)
        squares = jnp.sum(v * v, axis=-1, keepdims=True)
        for b in range(rows // span):
            here = pl.ds(pl.multiple_of(slot * rows + b * span, LANES), span)
            stat[mine, 0:1, here] = row_of(total[b * span : (b + 1) * span])
            stat[mine, 1:2, here] = row_of(squares[b * span : (b + 1) * span])

    def project_u(slot):
        u = dot(normed[slot], g0[...].reshape(depth, width)).astype(BF16).astype(F32)
        act_u[slot] = jax.nn.gelu(u)

    last = lines - 1

    @pl.loop(0, 4)
    def _(slot):
        project_v(slot)

        @pl.when(slot == 3)
        def _():
            crossed(2)
            for d in range(2, last):
                steps(1, d, at_end, (False,))

    for device in (across, twin, diag):
        remote(stat.at[mine], stat.at[mine], stat_send, stat_recv.at[mine], device).start()
    cross_pair(PHASES[2][0]).start()

    @pl.loop(0, 4)
    def _(slot):
        project_u(slot)

        @pl.when(slot == 1)
        def _():
            for d in range(2, last):
                steps(1, d, at_end, (True,))

    for s in PHASES[3]:
        cross_line(s).start()
    for other in (beside, peers, peers + 1):
        remote(
            stat.at[other], stat.at[other], stat_send, stat_recv.at[other], across
        ).wait_recv()

    gain_here = spatial_gain[:, pl.ds(pl.multiple_of(mine * width, LANES), width)]
    bias_here = spatial_bias[:, pl.ds(pl.multiple_of(mine * width, LANES), width)]
    pairs = heads // per

    def gate_slot(slot):
        low = []
        for b in range(rows // span):
            here = pl.ds(pl.multiple_of(slot * rows + b * span, LANES), span)
            sums = stat[0, :, here] + stat[1, :, here] + stat[2, :, here] + stat[3, :, here]
            mean_row = sums[0:1] / group
            var_row = sums[1:2] / group - mean_row * mean_row
            mean = column_of(mean_row)
            scale = lax.rsqrt(column_of(var_row) + 1e-05)
            v = act_v[slot, b * span : (b + 1) * span, :]
            vnorm = (v - mean) * scale * gain_here + bias_here
            parts = []
            for p in range(pairs):
                tile_v = vnorm[:, p * LANES : (p + 1) * LANES]
                parts.append(
                    jnp.concatenate(
                        [
                            jnp.where(lane // HEAD == k, tile_v, 0.0).astype(BF16)
                            for k in range(per)
                        ],
                        axis=0,
                    )
                )
            low.append(parts)
        for p in range(pairs):
            rhs = jnp.concatenate([parts[p] for parts in low], axis=1)
            mixed = dot(wcat[p], rhs)
            here = slice(p * LANES, (p + 1) * LANES)
            for b in range(rows // span):
                there = slice(b * span, (b + 1) * span)
                m = mixed[:, b * LANES : (b + 1) * LANES] + offs[:, here]
                gated[slot, there, here] = (act_u[slot, there, here] * m).astype(BF16)

    @pl.loop(0, 4)
    def _(slot):
        gate_slot(slot)

    model = g2.shape[2]
    def nth(i):
        d = (i + 1) // 2
        close = jnp.where(i % 2 == 1, q + d, q - d)
        far = jnp.where(q < lines - 1 - q, i, lines - 1 - i)
        return jnp.where(i <= 2 * near, close, far)

    def of_block(i):
        return 2 * nth(i // 2) + jnp.where(i % 2 == 0, y, 1 - y)

    def part_copy(b):
        return remote(part_out.at[b], part_in.at[b], part_send, part_recv.at[b], twin)

    def sum_copy(b):
        return remote(sum_out.at[b], sum_in.at[b], sum_send, sum_recv.at[b], across)

    def mid_copy(k, slot):
        return remote(
            middle.at[k, slot], middle.at[k, slot], mid_send, mid_recv.at[slot], twin
        )

    def mixer_product(first, b):
        lhs = gated[pl.ds(first, 2)].reshape(2 * rows, width)
        return dot(lhs, g2[b]).reshape(2, rows, model)

    @pl.loop(0, fs + 1)
    def _(i):
        @pl.when(i < fs)
        def _():
            b = of_block(i)

            @pl.when(b != f)
            def _():
                pair_wait(2, b)

            part_out[b] = mixer_product(peers, b).astype(BF16)
            part_copy(b).start()

        @pl.when(i > 0)
        def _():
            b = of_block(i - 1)
            value = mixer_product(c * 2, b)
            part_copy(b).wait_recv()
            sum_out[b] = (value + part_in[b].astype(F32)).astype(BF16)
            sum_copy(b).start()

        @pl.when(i == 1)
        def _():
            steps(1, last, at_end & (last > 1))

        @pl.when(i == 3)
        def _():
            steps(2, 1, inside, (False,))

        @pl.when(i == 5)
        def _():
            steps(2, 1, inside, (True,))

        @pl.when(i == fs // 2)
        def _():
            step(PHASES[2][0], 1, False, at_end)

        @pl.when(i == fs - 1)
        def _():
            step(PHASES[2][1], 1, False, at_end)

    for s in PHASES[2][1:] + PHASES[3]:
        cross_pair(s).start()

    @pl.loop(0, lines)
    def _(i):
        @pl.when(i == 0)
        def _():
            for d in range(2, lines):
                steps(2, d, inside, (False,))
            steps(2, 1, at_end, (True,))

        @pl.when(i == 1)
        def _():
            for d in range(2, lines):
                steps(2, d, inside, (True,))
            for d in range(2, last):
                steps(2, d, at_end, (False,))
            own(3)
            crossed(3)

        @pl.when(i == lines - 2)
        def _():
            for d in range(2, last):
                steps(2, d, at_end, (True,))
            steps(2, last, at_end & (last > 1), (False,))

        @pl.when(i == lines - 1)
        def _():
            for way in (from_right, from_left):
                for other in (False, True):
                    for s in PHASES[3]:
                        way(s, 1, other, inside)

            steps(2, last, at_end & (last > 1), (True,))

        k = nth(i)
        here = pl.ds(pl.multiple_of(k * 2 * model, LANES), 2 * model)
        for side in range(2):
            b = 2 * k + side
            sum_copy(b).wait_recv()
            for j in range(2):
                slot = c * 2 + j
                there = slice(side * model, (side + 1) * model)
                base = rows_in[slot, :, here][:, there].astype(F32)
                total = sum_out[b, j].astype(F32) + sum_in[b, j].astype(F32)
                middle[k, slot, :, there] = (base + total).astype(BF16)
        for j in range(2):
            mid_copy(k, c * 2 + j).start()

    def norm_middle(slot):
        @pl.loop(0, rows // tile)
        def _(i):
            here = pl.ds(pl.multiple_of(i * tile, tile), tile)
            wide = [middle[k, slot, here, :].astype(F32) for k in range(lines)]
            total = sum(jnp.sum(w * w, axis=-1, keepdims=True) for w in wide)
            scale = lax.rsqrt(total / depth + 1e-06)
            for k in range(lines):
                there = slice(k * 2 * model, (k + 1) * 2 * model)
                normed[slot, here, there] = (wide[k] * scale * channel_gain[:, there]).astype(BF16)

    steps_from(3, 2, inside)
    for j in range(2):
        norm_middle(c * 2 + j)
    for j in range(2):
        bulk(middle.at[:, peers + j], mid_recv.at[peers + j]).wait_recv()
        norm_middle(peers + j)

    steps(3, 1, at_end)
    for s in PHASES[2]:
        complete(s)

    def channel(slot):
        both = dot(normed[slot], g34[...].reshape(depth, 2 * units))
        pieces = [(0, main, 0, main)]
        if rest:
            pieces.append((main, units, 2 * main, 2 * main + rest))
        for first, end, gate_at, up_at in pieces:
            size = end - first
            gates = both[:, gate_at : gate_at + size].astype(BF16).astype(F32)
            ups = both[:, up_at : up_at + size].astype(BF16).astype(F32)
            place = lax.broadcasted_iota(jnp.int32, (rows, size), 0) % SEQ_LEN
            conv = taps_here[KCONV - 1 : KCONV, first:end] * gates
            for lag in range(1, KCONV):
                shifted = jnp.where(place >= lag, pltpu.roll(gates, lag, 0), 0.0)
                conv = conv + taps_here[KCONV - 1 - lag : KCONV - lag, first:end] * shifted
            hidden[slot, :, first:end] = (jax.nn.silu(conv) * ups).astype(BF16)

    bulk(part_out, part_send).wait_send()
    bulk(sum_out, sum_send).wait_send()

    def last_part(b, side):
        return remote(
            part_out.at[b, side],
            part_in.at[b, side],
            part_send2,
            part_recv2.at[b, side],
            twin,
        )

    def last_copy(b):
        return remote(sum_out.at[b, 0], last_in.at[b], last_send, last_recv.at[b], across)

    def give(b, side):
        part_out[b, side] = dot(hidden[peers + side], g5[b]).astype(BF16)
        last_part(b, side).start()

    def give_both(b):
        lhs = hidden[pl.ds(peers, 2)].reshape(2 * rows, units)
        part_out[b] = dot(lhs, g5[b]).reshape(2, rows, model).astype(BF16)
        for side in range(2):
            last_part(b, side).start()

    def pass_on(b):
        value = dot(hidden[beside], g5[b])
        last_part(b, 1 - y).wait_recv()
        sum_out[b, 0] = (value + part_in[b, 1 - y].astype(F32)).astype(BF16)
        last_copy(b).start()

    def send_blocks(first, end):
        @pl.loop(first, end)
        def _(i):
            b = of_block(i)
            pair_wait(5, b)
            give_both(b)
            pass_on(b)

    channel(1 - y)

    @pl.when(c == 1)
    def _():
        give(f, 1 - y)

    @pl.when(c == 0)
    def _():
        pass_on(f)

    for d in range(2, last):
        steps(3, d, at_end, (False,))
    channel(3 - y)

    @pl.when(c == 0)
    def _():
        give(f, 1 - y)

    pair_wait(5, beyond)
    give(beyond, 1 - y)

    @pl.when(c == 1)
    def _():
        pass_on(f)

    pass_on(beyond)
    early = min(4, fs)

    @pl.loop(2, early)
    def _(i):
        b = of_block(i)
        pair_wait(5, b)
        give(b, 1 - y)
        pass_on(b)

    for d in range(2, last):
        steps(3, d, at_end, (True,))
    most = (last,) if last > 1 else ()

    @pl.loop(0, 2)
    def _(core):
        channel(core * 2 + y)

        @pl.when(core == 0)
        def _():
            for d in most:
                steps(3, d, at_end, (False,))

    @pl.loop(0, early)
    def _(i):
        give(of_block(i), y)

    for d in most:
        steps(3, d, at_end, (True,))
    send_blocks(early, fs)

    def out_copy(k):
        here = pl.ds(pl.multiple_of(k * 2 * model, LANES), 2 * model)
        return pltpu.make_async_copy(out_here.at[k], out.at[:, here], out_sem.at[k])

    @pl.loop(0, lines)
    def _(i):
        k = nth(i)
        values = [dot(hidden[mine], g5[2 * k + side]) for side in range(2)]
        for side in range(2):
            b = 2 * k + side
            last_part(b, y).wait_recv()
            last_copy(b).wait_recv()
            total = values[side] + part_in[b, y].astype(F32) + last_in[b].astype(F32)
            there = slice(side * model, (side + 1) * model)
            total = total + middle[k, mine, :, there].astype(F32)
            out_here[k, :, there] = total.astype(BF16)
        out_copy(k).start()

    for s in range(STREAMS):
        chunks(s, 2, cross_send.at[s]).wait_send()
        chunks(s, fs - 2, pair_send.at[s]).wait_send()
    for k in range(lines):

        @pl.when(q == k)
        def _():
            for s in range(STREAMS):
                if k > 0:
                    chunks(s, 2 * (lines - k), left_send.at[s]).wait_send()
                if k < lines - 1:
                    chunks(s, 2 * (k + 1), right_send.at[s]).wait_send()

    bulk(rows_in.at[pl.ds(0, 3)], row_send).wait_send()
    bulk(stat.at[pl.ds(0, 3)], stat_send).wait_send()
    bulk(middle.at[:, pl.ds(0, 2)], mid_send).wait_send()
    bulk(part_out, part_send2).wait_send()
    bulk(last_in, last_send).wait_send()

    @pl.loop(0, lines)
    def _(k):
        out_copy(k).wait()


def body(reps, fs, tps):
    assert reps == 2 and tps == 2 and fs % 2 == 0

    def on_device(
        residual,
        mixer_gain,
        gating_proj,
        spatial_proj,
        spatial_gain,
        spatial_bias,
        spatial_mix,
        spatial_offset,
        mixer_out,
        channel_gain,
        gate_proj,
        up_proj,
        conv_taps,
        down_proj,
    ):
        rows, depth = residual.shape
        assert rows % SEQ_LEN == 0
        own_rows = gating_proj.shape[0]
        width = gating_proj.shape[1] // 2
        units = gate_proj.shape[1] // 2
        group = gating_proj.shape[1] * tps
        columns = mixer_out.shape[1]
        span = spatial_mix.shape[1]
        heads = width // HEAD
        lines = fs // 2
        vmem, hbm = pl.BlockSpec(memory_space=pltpu.VMEM), pl.BlockSpec(memory_space=pl.ANY)
        dma = pltpu.SemaphoreType.DMA
        return pl.pallas_call(
            functools.partial(kernel, (fs, rows, depth, group, width, units)),
            out_shape=jax.ShapeDtypeStruct((rows, depth), BF16),
            in_specs=[hbm] * 8 + [vmem] * 6,
            out_specs=hbm,
            scratch_shapes=[
                pltpu.VMEM((fs, own_rows, width), BF16),
                pltpu.VMEM((fs, own_rows, width), BF16),
                pltpu.VMEM((fs, width, columns), BF16),
                pltpu.VMEM((fs, own_rows, 2 * units), BF16),
                pltpu.VMEM((fs, units, columns), BF16),
                pltpu.VMEM((2, own_rows, 2 * units), BF16),
                pltpu.VMEM((own_rows, 2 * units), BF16),
                pltpu.VMEM((KCONV, units), F32),
                pltpu.VMEM((4, rows, depth), BF16),
                pltpu.VMEM((4, rows, depth), BF16),
                pltpu.VMEM((lines, 4, rows, 2 * columns), BF16),
                pltpu.VMEM((4, rows, width), F32),
                pltpu.VMEM((4, rows, width), F32),
                pltpu.VMEM((4, rows, width), BF16),
                pltpu.VMEM((4, rows, units), BF16),
                pltpu.VMEM((heads, span, span), BF16),
                pltpu.VMEM((heads * HEAD // LANES, span, span * LANES // HEAD), BF16),
                pltpu.VMEM((span, width), F32),
                pltpu.VMEM((4, 2, 4 * rows), F32),
                pltpu.VMEM((fs, 2, rows, columns), BF16),
                pltpu.VMEM((fs, 2, rows, columns), BF16),
                pltpu.VMEM((fs, 2, rows, columns), BF16),
                pltpu.VMEM((fs, 2, rows, columns), BF16),
                pltpu.VMEM((fs, rows, columns), BF16),
                pltpu.VMEM((lines, rows, 2 * columns), BF16),
                dma((STREAMS + 2,)),
                dma((lines,)),
                dma((STREAMS, fs)),
                dma((2, fs)),
                dma((STREAMS,)),
                dma((STREAMS,)),
                dma((STREAMS,)),
                dma((STREAMS,)),
                dma((STREAMS,)),
                dma(()),
                dma((4,)),
                dma(()),
                dma((4,)),
                dma(()),
                dma((fs,)),
                dma(()),
                dma((fs,)),
                dma(()),
                dma((4,)),
                dma(()),
                dma((fs, 2)),
                dma(()),
                dma((fs,)),
            ],
            compiler_params=pltpu.CompilerParams(
                collective_id=0, has_side_effects=True, vmem_limit_bytes=67043328
            ),
        )(
            residual,
            gating_proj,
            spatial_proj,
            mixer_out,
            gate_proj,
            up_proj,
            down_proj,
            spatial_mix,
            mixer_gain.reshape(1, -1),
            channel_gain.reshape(1, -1),
            spatial_gain.reshape(1, -1),
            spatial_bias.reshape(1, -1),
            spatial_offset,
            conv_taps,
        )

    return on_device


def solution(mesh):
    in_specs = (
        P(("rep", "fs", "tp"), None),
        P(),
        P("fs", "tp"),
        P("fs", "tp"),
        P(),
        P(),
        P(),
        P(),
        P("tp", "fs"),
        P(),
        P("fs", "tp"),
        P("fs", "tp"),
        P(),
        P("tp", "fs"),
    )
    out_specs = P(("rep", "fs", "tp"), None)
    return jax.shard_map(
        body(mesh.shape["rep"], mesh.shape["fs"], mesh.shape["tp"]),
        mesh=mesh,
        in_specs=in_specs,
        out_specs=out_specs,
        check_vma=False,
    )
```

```python
import functools

import jax
import jax.numpy as jnp
from jax import lax
from jax.experimental import pallas as pl
from jax.experimental.pallas import tpu as pltpu
from jax.sharding import PartitionSpec as P

HEAD = 64
SEGMENT = 64
KCONV = 3
SEQ_LEN = 256
LANES = 128

MESH = pl.DeviceIdType.MESH
BF16, F32 = jnp.bfloat16, jnp.float32

PHASES = ((0, 1), (2,), (3, 4), (5,))
STREAMS = 6


def dot(a, b):
    return jnp.dot(a, b, preferred_element_type=F32)


def kernel(
    dims,
    residual,
    gating,
    spatial,
    mixer_out,
    gate,
    up,
    down,
    mix,
    mixer_gain,
    channel_gain,
    spatial_gain,
    spatial_bias,
    offset,
    taps,
    out,
    g0,
    g1,
    g2,
    g34,
    g5,
    raw,
    cross,
    taps_here,
    rows_in,
    normed,
    middle,
    act_u,
    act_v,
    gated,
    hidden,
    mixw,
    wcat,
    offs,
    stat,
    part_out,
    part_in,
    sum_out,
    sum_in,
    last_in,
    out_here,
    local_sem,
    out_sem,
    line_recv,
    pair_each,
    pair_all,
    left_send,
    right_send,
    pair_send,
    cross_send,
    row_send,
    row_recv,
    stat_send,
    stat_recv,
    part_send,
    part_recv,
    sum_send,
    sum_recv,
    mid_send,
    mid_recv,
    part_send2,
    part_recv2,
    last_send,
    last_recv,
):
    fs, rows, depth, group, width, units = dims
    lines = fs // 2
    blocks = (g0, g1, g2, g34, g34, g5)
    halves = [block.shape[1] // 2 for block in blocks]
    sizes = [size // 2 if s in PHASES[2] else size for s, size in enumerate(halves)]
    starts = [sizes[s] if s == PHASES[2][1] else 0 for s in range(STREAMS)]
    r, f, c = lax.axis_index("rep"), lax.axis_index("fs"), lax.axis_index("tp")
    q, y = f // 2, f % 2
    beyond = f + 1 - 2 * y
    mine = c * 2 + y
    beside = c * 2 + 1 - y
    peers = (1 - c) * 2
    left, right = (r, f - 2, c), (r, f + 2, c)
    across, copy_chip = (r, beyond, c), (1 - r, f, c)
    twin, diag = (r, f, 1 - c), (r, beyond, 1 - c)
    has_left, has_right = q > 0, q < lines - 1

    def remote(src, dst, send, recv, device):
        return pltpu.make_async_remote_copy(
            src_ref=src,
            dst_ref=dst,
            send_sem=send,
            recv_sem=recv,
            device_id=device,
            device_id_type=MESH,
        )

    def at(start, size, step):
        return pl.ds(pl.multiple_of(start, step), size)

    own_copies = {
        0: (gating.at[:, at(y * width, width, LANES)], g0.at[f]),
        1: (spatial.at[:, at(y * width, width, LANES)], g1.at[f]),
        2: (mixer_out.at[at(y * width, width, 16)], g2.at[f]),
        3: (gate, raw.at[0]),
        4: (up, raw.at[1]),
        5: (down.at[at(y * units, units, 16)], g5.at[f]),
    }
    own_copies = [
        pltpu.make_async_copy(*own_copies[s], local_sem.at[s]) for s in range(STREAMS)
    ]
    heads = mixw.shape[0]
    head = mine * heads
    row_copy = pltpu.make_async_copy(residual, rows_in.at[mine], local_sem.at[STREAMS])
    mix_copy = pltpu.make_async_copy(mix.at[pl.ds(head, heads)], mixw, local_sem.at[STREAMS + 1])
    for copy in own_copies[:2] + [row_copy] + own_copies[2:] + [mix_copy]:
        copy.start()

    barrier = pltpu.get_barrier_semaphore()
    for device in (across, copy_chip, twin, diag):
        pl.semaphore_signal(barrier, inc=1, device_id=device, device_id_type=MESH)

    @pl.when(has_left)
    def _():
        pl.semaphore_signal(barrier, inc=1, device_id=left, device_id_type=MESH)

    @pl.when(has_right)
    def _():
        pl.semaphore_signal(barrier, inc=1, device_id=right, device_id_type=MESH)

    pl.semaphore_wait(barrier, 4 + jnp.minimum(q, 1) + jnp.minimum(lines - 1 - q, 1))

    def half(s, source, h):
        return blocks[s].at[source, at(h * halves[s] + starts[s], sizes[s], 16)]

    def on_line(s, source, send, device):
        ref = half(s, source, r)
        return remote(ref, ref, send, line_recv.at[s, source], device)

    def pair_sem(s, source):
        each = PHASES[1] + PHASES[3]
        return pair_each.at[each.index(s), source] if s in each else pair_all.at[s]

    def to_copy(s, source):
        ref = half(s, source, r)
        return remote(ref, ref, pair_send.at[s], pair_sem(s, source), copy_chip)

    def line_wait(s, source):
        on_line(s, source, left_send.at[s], across).wait_recv()

    def pair_wait(s, source):
        ref = half(s, source, 1 - r)
        remote(ref, ref, pair_send.at[s], pair_sem(s, source), copy_chip).wait_recv()

    def bulk(ref, sem):
        return remote(ref, ref, sem, sem, across)

    def chunks(s, count, sem):
        return bulk(blocks[s].at[pl.ds(0, count), pl.ds(0, sizes[s])], sem)

    def crossing(s, h):
        start = (1 - y) * width
        here = at(h * halves[s], halves[s], 16)
        if s < 2:
            src = (gating, spatial)[s].at[here, at(start, width, LANES)]
        elif s == 2:
            src = mixer_out.at[at(start + h * halves[s], halves[s], 16)]
        elif s < 5:
            src = cross.at[at(h * halves[s] + starts[s], sizes[s], 16)]
        else:
            src = down.at[at((1 - y) * units + h * halves[s], halves[s], 16)]
        return src, half(s, f, h)

    def cross_line(s):
        src, dst = crossing(s, r)
        return remote(src, dst, cross_send.at[s], line_recv.at[s, f], across)

    def cross_pair(s):
        src, dst = crossing(s, 1 - r)
        return remote(src, dst, cross_send.at[s], pair_sem(s, f), across)

    def both_ways(s, source):
        @pl.when(has_left)
        def _():
            on_line(s, source, left_send.at[s], left).start()

        @pl.when(has_right)
        def _():
            on_line(s, source, right_send.at[s], right).start()

    def own(p):
        for s in PHASES[p]:
            both_ways(s, f)

    def crossed(p, only=None):
        for s in PHASES[p] if only is None else (only,):
            line_wait(s, beyond)
            both_ways(s, beyond)

    near = jnp.minimum(q, lines - 1 - q)
    at_end, inside = near == 0, near > 0

    def from_left(s, d, other, who):
        @pl.when((q - d >= 0) & who)
        def _():
            source = (beyond if other else f) - 2 * d
            line_wait(s, source)

            @pl.when(has_right)
            def _():
                on_line(s, source, right_send.at[s], right).start()

            to_copy(s, source).start()

    def from_right(s, d, other, who):
        @pl.when((q + d < lines) & who)
        def _():
            source = (beyond if other else f) + 2 * d
            line_wait(s, source)

            @pl.when(has_left)
            def _():
                on_line(s, source, left_send.at[s], left).start()

            to_copy(s, source).start()

    def step(s, d, other, who):
        from_left(s, d, other, who)
        from_right(s, d, other, who)

    def steps(p, d, who=True, others=(False, True)):
        for other in others:
            for s in PHASES[p]:
                step(s, d, other, who)

    def steps_from(p, first, who):
        for d in range(first, lines):
            steps(p, d, who)

    def complete(s):
        chunks(s, fs - 1, pair_all.at[s]).wait_recv()

    row_to_across = remote(residual, rows_in.at[mine], row_send, row_recv.at[mine], across)
    row_to_twin = remote(residual, rows_in.at[mine], row_send, row_recv.at[mine], twin)
    for s in PHASES[0] + PHASES[1]:
        cross_line(s).start()
    row_to_across.start()
    row_to_twin.start()
    for s in PHASES[0]:
        cross_pair(s).start()
        own_copies[s].wait()
    own(0)

    def row_wait(slot):
        remote(
            rows_in.at[slot], rows_in.at[slot], row_send, row_recv.at[slot], across
        ).wait_recv()

    tile = 64

    def norm_in(slot):
        @pl.loop(0, rows // tile)
        def _(i):
            here = pl.ds(pl.multiple_of(i * tile, tile), tile)
            wide = rows_in[slot, here, :].astype(F32)
            scale = lax.rsqrt(jnp.mean(wide * wide, axis=-1, keepdims=True) + 1e-06)
            normed[slot, here, :] = (wide * scale * mixer_gain[...]).astype(BF16)

    main = units // LANES * LANES
    rest = units - main
    for s in PHASES[2]:
        own_copies[s].wait()
    for way in range(2):

        @pl.when(y == way)
        def _():
            for i in range(2):
                for ref, first in ((g34.at[f], way * units), (cross, (1 - way) * units)):
                    ref[:, i * main : (i + 1) * main] = raw[i, :, first : first + main]
                    if rest:
                        there = slice(2 * main + i * rest, 2 * main + (i + 1) * rest)
                        ref[:, there] = raw[i, :, first + main : first + units]

    for k in range(4):

        @pl.when(mine == k)
        def _():
            taps_here[...] = taps[:, k * units : (k + 1) * units]

    row_copy.wait()
    norm_in(mine)
    own_copies[2].wait()
    own_copies[5].wait()
    mix_copy.wait()

    for s in PHASES[0]:
        step(s, 1, False, True)
        crossed(0, s)
    for d in range(1, lines - 1):
        for s in PHASES[0]:
            step(s, d + 1, False, True)
            step(s, d, True, True)
    own(1)
    crossed(1)
    for s in PHASES[2]:
        cross_line(s).start()
    steps(0, lines - 1, True, (True,))
    row_wait(beside)
    row_forward = remote(
        rows_in.at[beside], rows_in.at[beside], row_send, row_recv.at[beside], twin
    )
    row_forward.start()
    norm_in(beside)
    for s in PHASES[1]:
        cross_pair(s).start()
    steps(1, 1, inside)
    for j in range(2):
        row_wait(peers + j)
        norm_in(peers + j)
    steps_from(1, 2, inside)
    own(2)
    steps(1, 1, at_end)

    span = mixw.shape[1]
    per = LANES // HEAD
    at_row = lax.broadcasted_iota(jnp.int32, (span, span), 0)
    at_col = lax.broadcasted_iota(jnp.int32, (span, span), 1)
    allowed = at_col // SEGMENT <= at_row // SEGMENT
    eye = at_col == at_row
    lane = lax.broadcasted_iota(jnp.int32, (span, LANES), 1)

    def column_of(row):
        return jnp.sum(
            jnp.where(eye, jnp.broadcast_to(row, (span, span)), 0.0), axis=1, keepdims=True
        )

    def row_of(column):
        return jnp.sum(
            jnp.where(eye, jnp.broadcast_to(column, (span, span)), 0.0), axis=0, keepdims=True
        )

    for p in range(heads // per):
        off = jnp.zeros((span, LANES), F32)
        for k in range(per):
            h = p * per + k
            wcat[p, :, k * span : (k + 1) * span] = jnp.where(
                allowed, mixw[h].astype(F32), 0.0
            ).astype(BF16)
            here = column_of(offset[pl.ds(head + h, 1), :])
            off = jnp.where(lane // HEAD == k, here, off)
        offs[:, p * LANES : (p + 1) * LANES] = off

    for s in PHASES[0]:
        complete(s)

    def project_v(slot):
        v = dot(normed[slot], g1[...].reshape(depth, width)).astype(BF16).astype(F32)
        v = jax.nn.gelu(v)
        act_v[slot] = v
        total = jnp.sum(v, axis=-1, keepdims=True)
        squares = jnp.sum(v * v, axis=-1, keepdims=True)
        for b in range(rows // span):
            here = pl.ds(pl.multiple_of(slot * rows + b * span, LANES), span)
            stat[mine, 0:1, here] = row_of(total[b * span : (b + 1) * span])
            stat[mine, 1:2, here] = row_of(squares[b * span : (b + 1) * span])

    def project_u(slot):
        u = dot(normed[slot], g0[...].reshape(depth, width)).astype(BF16).astype(F32)
        act_u[slot] = jax.nn.gelu(u)

    last = lines - 1

    @pl.loop(0, 4)
    def _(slot):
        project_v(slot)

        @pl.when(slot == 3)
        def _():
            crossed(2)
            for d in range(2, last):
                steps(1, d, at_end, (False,))

    for device in (across, twin, diag):
        remote(stat.at[mine], stat.at[mine], stat_send, stat_recv.at[mine], device).start()
    cross_pair(PHASES[2][0]).start()

    @pl.loop(0, 4)
    def _(slot):
        project_u(slot)

        @pl.when(slot == 1)
        def _():
            for d in range(2, last):
                steps(1, d, at_end, (True,))

    for s in PHASES[3]:
        cross_line(s).start()
    for other in (beside, peers, peers + 1):
        remote(
            stat.at[other], stat.at[other], stat_send, stat_recv.at[other], across
        ).wait_recv()

    gain_here = spatial_gain[:, pl.ds(pl.multiple_of(mine * width, LANES), width)]
    bias_here = spatial_bias[:, pl.ds(pl.multiple_of(mine * width, LANES), width)]
    pairs = heads // per

    def gate_slot(slot):
        low = []
        for b in range(rows // span):
            here = pl.ds(pl.multiple_of(slot * rows + b * span, LANES), span)
            sums = stat[0, :, here] + stat[1, :, here] + stat[2, :, here] + stat[3, :, here]
            mean_row = sums[0:1] / group
            var_row = sums[1:2] / group - mean_row * mean_row
            mean = column_of(mean_row)
            scale = lax.rsqrt(column_of(var_row) + 1e-05)
            v = act_v[slot, b * span : (b + 1) * span, :]
            vnorm = (v - mean) * scale * gain_here + bias_here
            parts = []
            for p in range(pairs):
                tile_v = vnorm[:, p * LANES : (p + 1) * LANES]
                parts.append(
                    jnp.concatenate(
                        [
                            jnp.where(lane // HEAD == k, tile_v, 0.0).astype(BF16)
                            for k in range(per)
                        ],
                        axis=0,
                    )
                )
            low.append(parts)
        for p in range(pairs):
            rhs = jnp.concatenate([parts[p] for parts in low], axis=1)
            mixed = dot(wcat[p], rhs)
            here = slice(p * LANES, (p + 1) * LANES)
            for b in range(rows // span):
                there = slice(b * span, (b + 1) * span)
                m = mixed[:, b * LANES : (b + 1) * LANES] + offs[:, here]
                gated[slot, there, here] = (act_u[slot, there, here] * m).astype(BF16)

    @pl.loop(0, 4)
    def _(slot):
        gate_slot(slot)

    model = g2.shape[2]
    def nth(i):
        d = (i + 1) // 2
        close = jnp.where(i % 2 == 1, q + d, q - d)
        far = jnp.where(q < lines - 1 - q, i, lines - 1 - i)
        return jnp.where(i <= 2 * near, close, far)

    def of_block(i):
        return 2 * nth(i // 2) + jnp.where(i % 2 == 0, y, 1 - y)

    def part_copy(b):
        return remote(part_out.at[b], part_in.at[b], part_send, part_recv.at[b], twin)

    def sum_copy(b):
        return remote(sum_out.at[b], sum_in.at[b], sum_send, sum_recv.at[b], across)

    def mid_copy(k, slot):
        return remote(
            middle.at[k, slot], middle.at[k, slot], mid_send, mid_recv.at[slot], twin
        )

    def mixer_product(first, b):
        lhs = gated[pl.ds(first, 2)].reshape(2 * rows, width)
        return dot(lhs, g2[b]).reshape(2, rows, model)

    @pl.loop(0, fs + 1)
    def _(i):
        @pl.when(i < fs)
        def _():
            b = of_block(i)

            @pl.when(b != f)
            def _():
                pair_wait(2, b)

            part_out[b] = mixer_product(peers, b).astype(BF16)
            part_copy(b).start()

        @pl.when(i > 0)
        def _():
            b = of_block(i - 1)
            value = mixer_product(c * 2, b)
            part_copy(b).wait_recv()
            sum_out[b] = (value + part_in[b].astype(F32)).astype(BF16)
            sum_copy(b).start()

        @pl.when(i == 1)
        def _():
            steps(1, last, at_end & (last > 1))

        @pl.when(i == 3)
        def _():
            steps(2, 1, inside, (False,))

        @pl.when(i == 5)
        def _():
            steps(2, 1, inside, (True,))

        @pl.when(i == fs // 2)
        def _():
            step(PHASES[2][0], 1, False, at_end)

        @pl.when(i == fs - 1)
        def _():
            step(PHASES[2][1], 1, False, at_end)

    for s in PHASES[2][1:] + PHASES[3]:
        cross_pair(s).start()

    @pl.loop(0, lines)
    def _(i):
        @pl.when(i == 0)
        def _():
            for d in range(2, lines):
                steps(2, d, inside, (False,))
            steps(2, 1, at_end, (True,))

        @pl.when(i == 1)
        def _():
            for d in range(2, lines):
                steps(2, d, inside, (True,))
            for d in range(2, last):
                steps(2, d, at_end, (False,))
            own(3)
            crossed(3)

        @pl.when(i == lines - 2)
        def _():
            for d in range(2, last):
                steps(2, d, at_end, (True,))
            steps(2, last, at_end & (last > 1), (False,))

        @pl.when(i == lines - 1)
        def _():
            for way in (from_right, from_left):
                for other in (False, True):
                    for s in PHASES[3]:
                        way(s, 1, other, inside)

            steps(2, last, at_end & (last > 1), (True,))

        k = nth(i)
        here = pl.ds(pl.multiple_of(k * 2 * model, LANES), 2 * model)
        for side in range(2):
            b = 2 * k + side
            sum_copy(b).wait_recv()
            for j in range(2):
                slot = c * 2 + j
                there = slice(side * model, (side + 1) * model)
                base = rows_in[slot, :, here][:, there].astype(F32)
                total = sum_out[b, j].astype(F32) + sum_in[b, j].astype(F32)
                middle[k, slot, :, there] = (base + total).astype(BF16)
        for j in range(2):
            mid_copy(k, c * 2 + j).start()

    def norm_middle(slot):
        @pl.loop(0, rows // tile)
        def _(i):
            here = pl.ds(pl.multiple_of(i * tile, tile), tile)
            wide = [middle[k, slot, here, :].astype(F32) for k in range(lines)]
            total = sum(jnp.sum(w * w, axis=-1, keepdims=True) for w in wide)
            scale = lax.rsqrt(total / depth + 1e-06)
            for k in range(lines):
                there = slice(k * 2 * model, (k + 1) * 2 * model)
                normed[slot, here, there] = (wide[k] * scale * channel_gain[:, there]).astype(BF16)

    steps_from(3, 2, inside)
    for j in range(2):
        norm_middle(c * 2 + j)
    for j in range(2):
        bulk(middle.at[:, peers + j], mid_recv.at[peers + j]).wait_recv()
        norm_middle(peers + j)

    steps(3, 1, at_end)
    for s in PHASES[2]:
        complete(s)

    def channel(slot):
        both = dot(normed[slot], g34[...].reshape(depth, 2 * units))
        pieces = [(0, main, 0, main)]
        if rest:
            pieces.append((main, units, 2 * main, 2 * main + rest))
        for first, end, gate_at, up_at in pieces:
            size = end - first
            gates = both[:, gate_at : gate_at + size].astype(BF16).astype(F32)
            ups = both[:, up_at : up_at + size].astype(BF16).astype(F32)
            place = lax.broadcasted_iota(jnp.int32, (rows, size), 0) % SEQ_LEN
            conv = taps_here[KCONV - 1 : KCONV, first:end] * gates
            for lag in range(1, KCONV):
                shifted = jnp.where(place >= lag, pltpu.roll(gates, lag, 0), 0.0)
                conv = conv + taps_here[KCONV - 1 - lag : KCONV - lag, first:end] * shifted
            hidden[slot, :, first:end] = (jax.nn.silu(conv) * ups).astype(BF16)

    bulk(part_out, part_send).wait_send()
    bulk(sum_out, sum_send).wait_send()

    def last_part(b, side):
        return remote(
            part_out.at[b, side],
            part_in.at[b, side],
            part_send2,
            part_recv2.at[b, side],
            twin,
        )

    def last_copy(b):
        return remote(sum_out.at[b, 0], last_in.at[b], last_send, last_recv.at[b], across)

    def give(b, side):
        part_out[b, side] = dot(hidden[peers + side], g5[b]).astype(BF16)
        last_part(b, side).start()

    def pass_on(b):
        value = dot(hidden[beside], g5[b])
        last_part(b, 1 - y).wait_recv()
        sum_out[b, 0] = (value + part_in[b, 1 - y].astype(F32)).astype(BF16)
        last_copy(b).start()

    def send_blocks(first, end):
        @pl.loop(first, end)
        def _(i):
            b = of_block(i)
            pair_wait(5, b)
            give(b, 1 - y)
            give(b, y)
            pass_on(b)

    channel(1 - y)

    @pl.when(c == 1)
    def _():
        give(f, 1 - y)

    @pl.when(c == 0)
    def _():
        pass_on(f)

    for d in range(2, last):
        steps(3, d, at_end, (False,))
    channel(3 - y)

    @pl.when(c == 0)
    def _():
        give(f, 1 - y)

    pair_wait(5, beyond)
    give(beyond, 1 - y)

    @pl.when(c == 1)
    def _():
        pass_on(f)

    pass_on(beyond)
    early = min(4, fs)

    @pl.loop(2, early)
    def _(i):
        b = of_block(i)
        pair_wait(5, b)
        give(b, 1 - y)
        pass_on(b)

    for d in range(2, last):
        steps(3, d, at_end, (True,))
    most = (last,) if last > 1 else ()

    @pl.loop(0, 2)
    def _(core):
        channel(core * 2 + y)

        @pl.when(core == 0)
        def _():
            for d in most:
                steps(3, d, at_end, (False,))

    @pl.loop(0, early)
    def _(i):
        give(of_block(i), y)

    for d in most:
        steps(3, d, at_end, (True,))
    send_blocks(early, fs)

    def out_copy(k):
        here = pl.ds(pl.multiple_of(k * 2 * model, LANES), 2 * model)
        return pltpu.make_async_copy(out_here.at[k], out.at[:, here], out_sem.at[k])

    @pl.loop(0, lines)
    def _(i):
        k = nth(i)
        values = [dot(hidden[mine], g5[2 * k + side]) for side in range(2)]
        for side in range(2):
            b = 2 * k + side
            last_part(b, y).wait_recv()
            last_copy(b).wait_recv()
            total = values[side] + part_in[b, y].astype(F32) + last_in[b].astype(F32)
            there = slice(side * model, (side + 1) * model)
            total = total + middle[k, mine, :, there].astype(F32)
            out_here[k, :, there] = total.astype(BF16)
        out_copy(k).start()

    for s in range(STREAMS):
        chunks(s, 2, cross_send.at[s]).wait_send()
        chunks(s, fs - 2, pair_send.at[s]).wait_send()
    for k in range(lines):

        @pl.when(q == k)
        def _():
            for s in range(STREAMS):
                if k > 0:
                    chunks(s, 2 * (lines - k), left_send.at[s]).wait_send()
                if k < lines - 1:
                    chunks(s, 2 * (k + 1), right_send.at[s]).wait_send()

    bulk(rows_in.at[pl.ds(0, 3)], row_send).wait_send()
    bulk(stat.at[pl.ds(0, 3)], stat_send).wait_send()
    bulk(middle.at[:, pl.ds(0, 2)], mid_send).wait_send()
    bulk(part_out, part_send2).wait_send()
    bulk(last_in, last_send).wait_send()

    @pl.loop(0, lines)
    def _(k):
        out_copy(k).wait()


def body(reps, fs, tps):
    assert reps == 2 and tps == 2 and fs % 2 == 0

    def on_device(
        residual,
        mixer_gain,
        gating_proj,
        spatial_proj,
        spatial_gain,
        spatial_bias,
        spatial_mix,
        spatial_offset,
        mixer_out,
        channel_gain,
        gate_proj,
        up_proj,
        conv_taps,
        down_proj,
    ):
        rows, depth = residual.shape
        assert rows % SEQ_LEN == 0
        own_rows = gating_proj.shape[0]
        width = gating_proj.shape[1] // 2
        units = gate_proj.shape[1] // 2
        group = gating_proj.shape[1] * tps
        columns = mixer_out.shape[1]
        span = spatial_mix.shape[1]
        heads = width // HEAD
        lines = fs // 2
        vmem, hbm = pl.BlockSpec(memory_space=pltpu.VMEM), pl.BlockSpec(memory_space=pl.ANY)
        dma = pltpu.SemaphoreType.DMA
        return pl.pallas_call(
            functools.partial(kernel, (fs, rows, depth, group, width, units)),
            out_shape=jax.ShapeDtypeStruct((rows, depth), BF16),
            in_specs=[hbm] * 8 + [vmem] * 6,
            out_specs=hbm,
            scratch_shapes=[
                pltpu.VMEM((fs, own_rows, width), BF16),
                pltpu.VMEM((fs, own_rows, width), BF16),
                pltpu.VMEM((fs, width, columns), BF16),
                pltpu.VMEM((fs, own_rows, 2 * units), BF16),
                pltpu.VMEM((fs, units, columns), BF16),
                pltpu.VMEM((2, own_rows, 2 * units), BF16),
                pltpu.VMEM((own_rows, 2 * units), BF16),
                pltpu.VMEM((KCONV, units), F32),
                pltpu.VMEM((4, rows, depth), BF16),
                pltpu.VMEM((4, rows, depth), BF16),
                pltpu.VMEM((lines, 4, rows, 2 * columns), BF16),
                pltpu.VMEM((4, rows, width), F32),
                pltpu.VMEM((4, rows, width), F32),
                pltpu.VMEM((4, rows, width), BF16),
                pltpu.VMEM((4, rows, units), BF16),
                pltpu.VMEM((heads, span, span), BF16),
                pltpu.VMEM((heads * HEAD // LANES, span, span * LANES // HEAD), BF16),
                pltpu.VMEM((span, width), F32),
                pltpu.VMEM((4, 2, 4 * rows), F32),
                pltpu.VMEM((fs, 2, rows, columns), BF16),
                pltpu.VMEM((fs, 2, rows, columns), BF16),
                pltpu.VMEM((fs, 2, rows, columns), BF16),
                pltpu.VMEM((fs, 2, rows, columns), BF16),
                pltpu.VMEM((fs, rows, columns), BF16),
                pltpu.VMEM((lines, rows, 2 * columns), BF16),
                dma((STREAMS + 2,)),
                dma((lines,)),
                dma((STREAMS, fs)),
                dma((2, fs)),
                dma((STREAMS,)),
                dma((STREAMS,)),
                dma((STREAMS,)),
                dma((STREAMS,)),
                dma((STREAMS,)),
                dma(()),
                dma((4,)),
                dma(()),
                dma((4,)),
                dma(()),
                dma((fs,)),
                dma(()),
                dma((fs,)),
                dma(()),
                dma((4,)),
                dma(()),
                dma((fs, 2)),
                dma(()),
                dma((fs,)),
            ],
            compiler_params=pltpu.CompilerParams(
                collective_id=0, has_side_effects=True, vmem_limit_bytes=67043328
            ),
        )(
            residual,
            gating_proj,
            spatial_proj,
            mixer_out,
            gate_proj,
            up_proj,
            down_proj,
            spatial_mix,
            mixer_gain.reshape(1, -1),
            channel_gain.reshape(1, -1),
            spatial_gain.reshape(1, -1),
            spatial_bias.reshape(1, -1),
            spatial_offset,
            conv_taps,
        )

    return on_device


def solution(mesh):
    in_specs = (
        P(("rep", "fs", "tp"), None),
        P(),
        P("fs", "tp"),
        P("fs", "tp"),
        P(),
        P(),
        P(),
        P(),
        P("tp", "fs"),
        P(),
        P("fs", "tp"),
        P("fs", "tp"),
        P(),
        P("tp", "fs"),
    )
    out_specs = P(("rep", "fs", "tp"), None)
    return jax.shard_map(
        body(mesh.shape["rep"], mesh.shape["fs"], mesh.shape["tp"]),
        mesh=mesh,
        in_specs=in_specs,
        out_specs=out_specs,
        check_vma=False,
    )
```
